32 devices in a mesh: grp: 2 (over x), ep: 16 (over z, y, core).
Axes of the slice: x: 2, y: 2, z: 4, core: 2. Of those that a mesh axis runs over, the one named last changes fastest.
Arguments:
- queries: bfloat16 [32, 8, 128], P(('grp', 'ep')), parts along dimension 0, may hold values from -400 to 400
- fresh_token_key: bfloat16 [32, 2, 128], P(('grp', 'ep')), parts along dimension 0, may hold values from -6 to 6
- value_new: bfloat16 [32, 2, 128], P(('grp', 'ep')), parts along dimension 0, may hold values from -6 to 6
- forget_logit: float32 [32, 8], P(('grp', 'ep')), parts along dimension 0, may hold values from -8 to 8
- cache_keys: bfloat16 [32, 2, 4096, 128], P(('grp', 'ep')), parts along dimension 0, may hold values from -12 to 12
- cache_values: bfloat16 [32, 2, 4096, 128], P(('grp', 'ep')), parts along dimension 0, may hold values from -6 to 6
- cache_cumlog: float32 [32, 8, 4096], P(('grp', 'ep')), parts along dimension 0, may hold values from -572 to 0
- lengths: int32 [32], P(('grp', 'ep')), parts along dimension 0, may hold values from 1024 to 4096
- residual: bfloat16 [32, 2048], P('grp', 'ep'), parts along dimension 0, may hold values from -6 to 6
- out_weight: bfloat16 [1024, 2048], P(None, 'ep'), may hold values from -0.1875 to 0.1875
- norm_gain: float32 [2048], replicated, may hold values from 0.1 to 1.9
- expert_gate: bfloat16 [16, 704, 2048], P('ep'), may hold values from -0.125 to 0.125
- expert_up: bfloat16 [16, 704, 2048], P('ep'), may hold values from -0.125 to 0.125
- expert_down: bfloat16 [16, 704, 2048], P('ep'), may hold values from -0.21875 to 0.21875
- shared_gate: bfloat16 [1408, 2048], P('ep'), may hold values from -0.125 to 0.125
- shared_up: bfloat16 [1408, 2048], P('ep'), may hold values from -0.125 to 0.125
- shared_down: bfloat16 [1408, 2048], P(None, 'ep'), may hold values from -0.15625 to 0.15625
- routes: int32 [32, 6], P('grp'), parts along dimension 0, may hold values from 0 to 15, all different within a row; in each aligned block of 16 rows (0 to 15, 16 to 31, ...) at most 12 rows name the same one
- route_scores: float32 [32, 6], P('grp'), parts along dimension 0, may hold values from 0.05 to 1
Outputs:
- updated: bfloat16 [32, 2048], P('grp', 'ep'), parts along dimension 0
The draws below stay inside these ranges and needn't reach their ends.
There are 2 independent parts, one for each index of `grp`. The reference program is written for one: setup_inputs(seed, part) draws one part's arguments, and reference() takes and returns one part's arrays. A program takes and returns all parts, laid end to end along the dimension named above; an argument that names none is the same for every part. Nothing has to cross between parts.
Inputs may be any that keep to these rules, and one draw needn't show every extreme that they name: `routes`: each row names 6 different experts; no expert is named by more than 12 rows of a part, a bound that some block reaches.
All inputs are finite; a program needn't handle non-finite values.
Results may differ from the reference program's by a relative error of at most 0.0068.
Values may be sent and summed in bfloat16 or wider, within the bound.
A program may use at most 64 MiB of HBM per device.

```python
import math
import jax
import jax.numpy as jnp
import numpy as np
from jax import lax

D = 2048
QUERY_HEADS = 8
HD = 128
KVH = 2
FF = 704
SHARED_FF = 1408
TOP_K = 6
CACHE_POSITIONS = 4096
SEQUENCE_TOTAL = 16
EXPERTS = 16
CAP = 12
QW = 1024


def draw_queries(key, part):
    sampled = jnp.clip(jax.random.normal(jax.random.fold_in(key, 511), (SEQUENCE_TOTAL, QUERY_HEADS, HD), jnp.float32), -6.0, 6.0)
    return sampled.astype(jnp.bfloat16)


def draw_cache_keys(key, part):
    sampled = jnp.clip(jax.random.normal(jax.random.fold_in(key, 521), (SEQUENCE_TOTAL, KVH, CACHE_POSITIONS, HD), jnp.float32), -6.0, 6.0)
    return sampled.astype(jnp.bfloat16)


def draw_cache_cumlog(key, part):
    slow_share = 0.5
    slow_heads = jax.random.uniform(jax.random.fold_in(key, 531), (SEQUENCE_TOTAL, QUERY_HEADS), jnp.float32) < slow_share
    seq_factor = 2.0 ** jax.random.uniform(jax.random.fold_in(key, 532), (SEQUENCE_TOTAL, 1, 1), jnp.float32, -1.0, 1.0)
    decay_rate = jnp.where(slow_heads, 1.0 / CACHE_POSITIONS, 1.0 / 40.0)[:, :, None] * seq_factor
    jitter_strength = jax.random.uniform(jax.random.fold_in(key, 533), (SEQUENCE_TOTAL, QUERY_HEADS, CACHE_POSITIONS), jnp.float32, 0.2, 1.8)
    cluster_positions = jax.random.uniform(jax.random.fold_in(key, 534), (SEQUENCE_TOTAL, 1, CACHE_POSITIONS), jnp.float32) < 4.0 / CACHE_POSITIONS
    cluster_length = jnp.log(jax.random.uniform(jax.random.fold_in(key, 535), (SEQUENCE_TOTAL, QUERY_HEADS, CACHE_POSITIONS), jnp.float32, 0.5, 0.8))
    step_log_gate = -decay_rate * jitter_strength + jnp.where(cluster_positions, cluster_length, 0.0)
    return jnp.cumsum(step_log_gate, axis=2)


def set_ends(result, stream_key, smallest, high):
    extent = result.shape
    index_at = [jax.random.randint(jax.random.fold_in(stream_key, axis), (), 0, extent[axis]) for axis in range(len(extent))]
    result = result.at[tuple(index_at)].set(smallest)
    longest = extent.index(max(extent))
    index_at[longest] = (index_at[longest] + 1) % extent[longest]
    return result.at[tuple(index_at)].set(high)


def block_scale(rng, shape, split, smallest, high):
    def one(dim, parts):
        steps = jax.random.uniform(jax.random.fold_in(jax.random.fold_in(rng, 6), dim), (parts,), jnp.float32, smallest / len(split), high / len(split))
        return jnp.repeat(jnp.exp(steps), shape[dim] // parts).reshape((-1,) + (1,) * (len(shape) - dim - 1))

    loudness = one(*split[0])
    for cut in split[1:]:
        loudness = loudness * one(*cut)
    return loudness


def deal_out(key, own, number, rows, amount, top, bound, skew):
    sequence = jax.random.permutation(key, amount)
    crowded, usual = shares(amount, rows * top, bound, skew, True), shares(amount, rows * top, bound, skew, False)
    places = jnp.arange(amount)

    def named(tallies, turn):
        used = int((tallies > 0).sum())
        fixed = max(1, used // 4)
        passed = fixed + (places - fixed + turn * (used - fixed)) % max(1, amount - fixed)
        return jnp.zeros((amount,), jnp.int32).at[sequence[jnp.where(places < fixed, places, passed)]].set(jnp.asarray(tallies, jnp.int32))

    tallies = jnp.where(number % 4 == 0, named(crowded, number // 4), named(usual, number - number // 4 - 1))
    mixed = jax.random.permutation(jax.random.fold_in(own, 3), amount)
    source_of, receiver = mixed[0:amount // 2 * 2:2], mixed[1:amount // 2 * 2:2]
    slack = jnp.minimum(tallies[source_of] - 1, bound - tallies[receiver]) // 2
    slack = jnp.where((source_of == sequence[0]) | (receiver == sequence[0]) | (tallies[receiver] == 0), 0, jnp.maximum(slack, 0))
    passed = jax.random.randint(jax.random.fold_in(own, 4), (amount // 2,), 0, 1 << 20) % (slack + 1)
    tallies = tallies.at[source_of].add(-passed).at[receiver].add(passed)
    labels = jnp.searchsorted(jnp.cumsum(tallies), jnp.arange(rows * top), side="right").astype(jnp.int32)
    table = labels.reshape(top, rows).T
    table = table[jax.random.permutation(jax.random.fold_in(own, 1), rows)]
    turn = jax.random.randint(jax.random.fold_in(own, 2), (rows, 1), 0, top)
    return jnp.take_along_axis(table, (jnp.arange(top)[None, :] + turn) % top, axis=1)


def shares(number_of, total, reach, skew, full):
    weights = [(1 << 20) // math.isqrt(grade ** skew) + 1 for grade in range(1, number_of + 1)]
    largest = reach if full else min(reach, max(-(-total // number_of), total * weights[0] // sum(weights)))
    least = 1 if total - largest >= number_of - 1 else 0
    counts, surplus = [largest] + [least] * (number_of - 1), total - largest - least * (number_of - 1)
    while surplus > 0:
        movable = [i for i in range(1, number_of) if counts[i] < largest] or [i for i in range(1, number_of) if counts[i] < reach]
        mass, remaining = sum([weights[i] for i in movable]), surplus
        for i in movable:
            more = min(reach - counts[i], max(1, remaining * weights[i] // mass), surplus)
            counts[i] = counts[i] + more
            surplus = surplus - more
    return np.array(counts)


def gaussian(rng, dims, width, most, split=(), held_as=jnp.bfloat16):
    array = jax.random.normal(rng, dims, jnp.float32) * width
    if len(split) > 0:
        array = block_scale(rng, dims, split, -0.22, 0.18) * array
    return jnp.clip(array, min=-most, max=most).astype(held_as)


def setup_inputs(seed: int = 0, part: int = 0) -> dict:
    splits = jax.random.split(jax.random.key(seed), 20)
    own_keys = jax.random.split(jax.random.fold_in(splits[19], part), 20)
    queries = draw_queries(jax.random.fold_in(jax.random.fold_in(splits[19], part), 71), part)
    fresh_token_key = gaussian(own_keys[1], (SEQUENCE_TOTAL, KVH, HD), 1.0, 6.0, ((0, 16),))
    value_new = gaussian(own_keys[2], (SEQUENCE_TOTAL, KVH, HD), 1.0, 6.0, ((0, 16),))
    forget_logit = gaussian(own_keys[3], (SEQUENCE_TOTAL, QUERY_HEADS), 2.0, 8.0, ((0, 16),), jnp.float32)
    cache_keys = draw_cache_keys(jax.random.fold_in(jax.random.fold_in(splits[19], part), 71), part)
    cache_values = gaussian(own_keys[5], (SEQUENCE_TOTAL, KVH, CACHE_POSITIONS, HD), 1.0, 6.0, ((0, 16),))
    cache_cumlog = draw_cache_cumlog(jax.random.fold_in(jax.random.fold_in(splits[19], part), 71), part)
    lengths = set_ends(jax.random.randint(own_keys[7], (SEQUENCE_TOTAL,), CACHE_POSITIONS // 4, CACHE_POSITIONS + 1), jax.random.fold_in(own_keys[7], 1), CACHE_POSITIONS // 4, CACHE_POSITIONS).astype(jnp.int32)
    residual = gaussian(own_keys[8], (SEQUENCE_TOTAL, D), 1.0, 6.0, ((1, 16),))
    out_weight = gaussian(splits[9], (QW, D), QW ** -0.5, 0.1875, ((1, 16),))
    norm_gain = jnp.clip(1.0 + 0.18 * jax.random.normal(splits[10], (D,), jnp.float32), 0.1, 1.9)
    expert_gate = gaussian(splits[11], (EXPERTS, FF, D), D ** -0.5, 0.125, ((0, 16),))
    expert_up = gaussian(splits[12], (EXPERTS, FF, D), D ** -0.5, 0.125, ((0, 16),))
    expert_down = gaussian(splits[13], (EXPERTS, FF, D), FF ** -0.5, 0.21875, ((0, 16),))
    shared_gate = gaussian(splits[14], (SHARED_FF, D), D ** -0.5, 0.125, ((0, 16),))
    shared_up = gaussian(splits[15], (SHARED_FF, D), D ** -0.5, 0.125, ((0, 16),))
    shared_down = gaussian(splits[16], (SHARED_FF, D), SHARED_FF ** -0.5, 0.15625, ((1, 16),))
    routes_keys = jax.random.split(jax.random.fold_in(own_keys[17], 1), SEQUENCE_TOTAL // SEQUENCE_TOTAL)
    routes_turns = jax.random.permutation(jax.random.fold_in(own_keys[17], 3), SEQUENCE_TOTAL // SEQUENCE_TOTAL)
    routes = jax.vmap(lambda own, number: deal_out(jax.random.fold_in(own_keys[17], 2), own, number, SEQUENCE_TOTAL, EXPERTS, TOP_K, CAP, 2))(routes_keys, routes_turns).reshape((SEQUENCE_TOTAL, TOP_K))
    route_scores = jnp.clip(jax.random.uniform(own_keys[18], (SEQUENCE_TOTAL, TOP_K), jnp.float32, 0.05, 1.0), 0.05, 1.0)
    return dict(queries=queries, fresh_token_key=fresh_token_key, value_new=value_new, forget_logit=forget_logit, cache_keys=cache_keys, cache_values=cache_values, cache_cumlog=cache_cumlog, lengths=lengths, residual=residual, out_weight=out_weight, norm_gain=norm_gain, expert_gate=expert_gate, expert_up=expert_up, expert_down=expert_down, shared_gate=shared_gate, shared_up=shared_up, shared_down=shared_down, routes=routes, route_scores=route_scores)


norm_eps = 1e-06
routed_scale = 2.5
contract_last = (((1,), (1,)), ((), ()))

def expert_hidden(row_block, gate_matrix, up_matrix):
    gate_part = lax.dot_general(row_block, gate_matrix, contract_last, preferred_element_type=jnp.float32)
    up_part = lax.dot_general(row_block, up_matrix, contract_last, preferred_element_type=jnp.float32)
    return (jax.nn.silu(gate_part) * up_part).astype(jnp.bfloat16)

def attend_one(packed):
    queries, fresh_token_key, value_new, forget_logit, cache_keys, cache_values, cache_cumlog, length = packed
    head_count, head_size = queries.shape
    key_heads, cache_span, _ = cache_keys.shape
    groups = head_count // key_heads
    inv_root = head_size ** (-0.5)
    grouped_heads = queries.astype(jnp.float32).reshape(key_heads, groups, head_size)
    scores = jnp.einsum('kgd,kpd->kgp', grouped_heads, cache_keys.astype(jnp.float32)).reshape(head_count, cache_span) * inv_root
    positions = jnp.arange(cache_span, dtype=jnp.int32)[None, :]
    latest = lax.optimization_barrier(jnp.sum(jnp.where(positions == length - 1, cache_cumlog, jnp.zeros_like(cache_cumlog)), axis=1))
    log_gate = jax.nn.log_sigmoid(forget_logit)
    scores = scores + (latest + log_gate)[:, None] - cache_cumlog
    visible = positions < length
    scores = jnp.where(visible, scores, -jnp.inf)
    own_score = jnp.einsum('kgd,kd->kg', grouped_heads, fresh_token_key.astype(jnp.float32)).reshape(head_count) * inv_root
    top_score = jnp.maximum(lax.optimization_barrier(jnp.max(scores, axis=1)), own_score)
    weights = jnp.where(visible, jnp.exp(scores - top_score[:, None]), jnp.zeros_like(scores))
    own_weight = jnp.exp(own_score - top_score)
    denominator = lax.optimization_barrier(jnp.sum(weights, axis=1)) + own_weight
    rounded = lax.optimization_barrier(weights.astype(jnp.bfloat16)).astype(jnp.float32)
    own_rounded = lax.optimization_barrier(own_weight.astype(jnp.bfloat16)).astype(jnp.float32)
    weighted = jnp.einsum('kgp,kpd->kgd', rounded.reshape(key_heads, groups, cache_span), cache_values.astype(jnp.float32)).reshape(head_count, head_size)
    own_value = jnp.repeat(value_new.astype(jnp.float32), groups, axis=0)
    numerator = weighted + own_rounded[:, None] * own_value
    return (numerator / denominator[:, None]).astype(jnp.bfloat16).reshape(head_count * head_size)

def reference(queries, fresh_token_key, value_new, forget_logit, cache_keys, cache_values, cache_cumlog, lengths, residual, out_weight, norm_gain, expert_gate, expert_up, expert_down, shared_gate, shared_up, shared_down, routes, route_scores):
    attended = lax.map(attend_one, (queries, fresh_token_key, value_new, forget_logit, cache_keys, cache_values, cache_cumlog, lengths))
    mixed = jnp.dot(attended, out_weight, preferred_element_type=jnp.float32)
    stream = (residual.astype(jnp.float32) + mixed).astype(jnp.bfloat16)
    rows_wide = stream.astype(jnp.float32)
    inv_rms = lax.rsqrt(lax.optimization_barrier(jnp.mean(rows_wide * rows_wide, axis=1, keepdims=True)) + norm_eps)
    normed = (rows_wide * inv_rms * norm_gain).astype(jnp.bfloat16)
    gate_weights = route_scores / lax.optimization_barrier(jnp.sum(route_scores, axis=1, keepdims=True)) * routed_scale
    slot_ids = jnp.arange(CAP, dtype=jnp.int32)[:, None]

    def one_expert(totals, packed):
        expert_id, gate_matrix, up_matrix, down_matrix = packed
        expert_hits = routes == expert_id
        is_member = lax.optimization_barrier(jnp.sum(expert_hits.astype(jnp.int32), axis=1)).astype(jnp.int32)
        token_share = lax.optimization_barrier(jnp.sum(jnp.where(expert_hits, gate_weights, jnp.zeros_like(gate_weights)), axis=1))
        slot_rank = (jnp.cumsum(is_member) - 1).astype(jnp.int32)
        selector = (is_member[None, :] == 1) & (slot_rank[None, :] == slot_ids)
        picked = jnp.dot(selector.astype(jnp.bfloat16), normed, preferred_element_type=jnp.float32).astype(jnp.bfloat16)
        hidden = expert_hidden(picked, gate_matrix, up_matrix)
        expert_out = jnp.dot(hidden, down_matrix, preferred_element_type=jnp.float32).astype(jnp.bfloat16)
        slot_share = jnp.dot(selector.astype(jnp.float32), token_share, precision=lax.Precision.HIGHEST)
        contribution = jnp.dot(selector.astype(jnp.float32).T, expert_out.astype(jnp.float32) * slot_share[:, None], precision=lax.Precision.HIGHEST)
        return (totals + contribution, None)
    routed, _ = lax.scan(one_expert, jnp.zeros(stream.shape, jnp.float32), (jnp.arange(EXPERTS, dtype=jnp.int32), expert_gate, expert_up, expert_down))
    shared_mid = expert_hidden(normed, shared_gate, shared_up)
    shared = jnp.dot(shared_mid, shared_down, preferred_element_type=jnp.float32)
    return (stream.astype(jnp.float32) + routed + shared).astype(jnp.bfloat16)
```

```python
import functools

import jax
import jax.numpy as jnp
from jax import lax
from jax.experimental import pallas as pl
from jax.experimental.pallas import tpu as pltpu
from jax.sharding import PartitionSpec as P

norm_eps = 1e-06
routed_scale = 2.5
contract_last = (((1,), (1,)), ((), ()))
LANES = 128
VMEM_LIMIT = 48 * 1024 * 1024
f32 = jnp.float32
bf16 = jnp.bfloat16


def dot_t(a, b):
    return lax.dot_general(a, b, contract_last, preferred_element_type=f32)


def join_lanes(blocks, width):
    if width % LANES == 0:
        return jnp.concatenate([b.astype(bf16) for b in blocks], axis=1)
    rows = blocks[0].shape[0]
    total = len(blocks) * width
    lane = lax.broadcasted_iota(jnp.int32, (rows, LANES), 1)
    pieces = [jnp.zeros((rows, LANES), f32) for _ in range(-(-total // LANES))]
    for k, block in enumerate(blocks):
        at, shift = divmod(k * width, LANES)
        moved = jnp.where(lane < width, block.astype(f32), 0.0)
        if shift:
            moved = pltpu.roll(moved, shift, 1)
        if shift + width <= LANES:
            pieces[at] = pieces[at] + moved
        else:
            pieces[at] = pieces[at] + jnp.where(lane >= shift, moved, 0.0)
            pieces[at + 1] = pieces[at + 1] + jnp.where(lane < shift, moved, 0.0)
    return jnp.concatenate([p.astype(bf16) for p in pieces], axis=1)[:, :total]


def widen(block):
    rows, width = block.shape
    short = -width % LANES
    if not short:
        return block
    return jnp.concatenate([block, jnp.zeros((rows, short), block.dtype)], axis=1)


def layer(
    n,
    lengths_hbm,
    q_hbm,
    fresh_hbm,
    vnew_hbm,
    forget_hbm,
    residual_hbm,
    gain_hbm,
    routes_hbm,
    route_scores_hbm,
    keys_hbm,
    values_hbm,
    cumlog_hbm,
    out_w_hbm,
    gate_hbm,
    up_hbm,
    down_hbm,
    sgate_hbm,
    sup_hbm,
    sdown_hbm,
    out_ref,
    lengths_ref,
    q_ref,
    fresh_ref,
    vnew_ref,
    forget_ref,
    residual_ref,
    gain_ref,
    routes_ref,
    route_scores_ref,
    keys,
    values,
    cumlog,
    out_w,
    gate_up_w,
    down_w,
    shared_w,
    sdown_w,
    att_buf,
    att_wide,
    stream_buf,
    mid_buf,
    eo_src,
    eo_buf,
    small_sem,
    load_sem,
    key_sem,
    value_sem,
    send_sem,
    recv_sem,
    stream_sem,
):
    me = lax.axis_index("ep")
    heads, head_size = q_ref.shape[1:]
    key_heads, span = keys.shape[:2]
    groups = heads // key_heads
    rows, width = residual_ref.shape
    ff, model = gate_up_w.shape[1:]
    shared_width = shared_w.shape[1]
    chunks = key_sem.shape[0]
    chunk = span // chunks

    def key_copy(c):
        part = pl.ds(c * chunk, chunk)
        return pltpu.make_async_copy(keys_hbm.at[0, :, part], keys.at[:, part], key_sem.at[c])

    def value_copy(c):
        part = pl.ds(c * chunk, chunk)
        return pltpu.make_async_copy(values_hbm.at[0, :, part], values.at[:, part], value_sem.at[c])

    cumlog_copy = pltpu.make_async_copy(cumlog_hbm.at[0], cumlog, load_sem.at[0])
    out_w_copy = pltpu.make_async_copy(out_w_hbm, out_w, load_sem.at[1])
    down_copy = pltpu.make_async_copy(down_hbm.at[0], down_w, load_sem.at[4])
    sdown_copy = pltpu.make_async_copy(sdown_hbm, sdown_w, load_sem.at[5])

    def pair_copies(first, second, both, sem):
        return [
            pltpu.make_async_copy(src, both.at[k], sem) for k, src in enumerate((first, second))
        ]

    shared_copies = pair_copies(sgate_hbm, sup_hbm, shared_w, load_sem.at[2])
    gate_up_copies = pair_copies(gate_hbm.at[0], up_hbm.at[0], gate_up_w, load_sem.at[3])

    smalls = [
        pltpu.make_async_copy(src, dst, small_sem.at[i])
        for i, (src, dst) in enumerate(
            (
                (q_hbm, q_ref),
                (fresh_hbm, fresh_ref),
                (vnew_hbm, vnew_ref),
                (forget_hbm, forget_ref),
                (lengths_hbm, lengths_ref),
                (routes_hbm, routes_ref),
                (route_scores_hbm, route_scores_ref),
                (residual_hbm, residual_ref),
                (gain_hbm, gain_ref),
            )
        )
    ]
    for copy in smalls[:5]:
        copy.start()
    cumlog_copy.start()
    for c in range(chunks):
        key_copy(c).start()
    for c in range(1):
        value_copy(c).start()

    barrier = pltpu.get_barrier_semaphore()

    def greet(i, carry):
        pl.semaphore_signal(barrier, inc=1, device_id={"ep": lax.rem(me + i, n)})
        return carry

    with jax.named_scope("greet"):
        lax.fori_loop(1, n, greet, 0)

    wide = max(width, 2 * LANES)
    per = wide // width
    turns = model // wide
    home = me // per
    toward = 1 - 2 * (home // (turns // 2))

    def remote(phase, src, dst, peer, sem):
        return pltpu.make_async_remote_copy(
            src_ref=src,
            dst_ref=dst,
            send_sem=send_sem.at[phase],
            recv_sem=sem,
            device_id={"ep": peer},
        )

    def spread(phase, buf, sem, order=""):
        def one(i, carry):
            if order == "asc":
                peer = i - 1 + (i - 1 + n - me) // n
            elif order == "desc":
                peer = n - i - jnp.where(n - i <= me, 1, 0)
            elif order == "near":
                peer = lax.rem(me + toward * i + n, n)
            else:
                peer = lax.rem(me + toward * (n - i) + n, n)
            remote(phase, buf.at[me], buf.at[me], peer, sem).start()
            return carry

        lax.fori_loop(1, n, one, 0)

    def arrive(phase, buf, sem, first, count):
        blocks = buf.at[pl.ds(first, count)]
        remote(phase, blocks, blocks, me, sem).wait_recv()

    def sent(phase, buf):
        blocks = buf.at[pl.ds(0, n - 1)]
        remote(phase, blocks, blocks, me, recv_sem.at[0]).wait_send()

    def visit(i):
        wrapped = (home + i) // turns
        return (1 - wrapped) * (home + i) + wrapped * (turns - 1 - i)

    with jax.named_scope("smallwait"):
        for copy in smalls[:5]:
            copy.wait()
    inv_root = head_size ** (-0.5)
    length = lengths_ref[0, 0]
    q = q_ref[0]
    head_row = lax.broadcasted_iota(jnp.int32, (heads, head_size), 0)
    q_wide = jnp.concatenate(
        [jnp.where(head_row // groups == k, q, jnp.zeros_like(q)) for k in range(key_heads)], axis=1
    )
    fresh, vnew = fresh_ref[0].astype(f32), vnew_ref[0].astype(f32)
    own_key, own_value = fresh[0:1], vnew[0:1]
    for k in range(1, key_heads):
        own_key = jnp.where(head_row // groups == k, fresh[k : k + 1], own_key)
        own_value = jnp.where(head_row // groups == k, vnew[k : k + 1], own_value)
    own_score = jnp.sum(q.astype(f32) * own_key, axis=1, keepdims=True) * inv_root
    eye = lax.broadcasted_iota(jnp.int32, (heads, heads), 0) == lax.broadcasted_iota(
        jnp.int32, (heads, heads), 1
    )
    forget = jnp.sum(jnp.where(eye, forget_ref[...], 0.0), axis=1, keepdims=True)
    log_gate = jnp.minimum(forget, 0.0) - jnp.log1p(jnp.exp(-jnp.abs(forget)))

    place = lax.broadcasted_iota(jnp.int32, (heads, chunk), 1)

    def both(ref, c):
        part = slice(c * chunk, (c + 1) * chunk)
        return jnp.concatenate([ref[k, part] for k in range(key_heads)], axis=1)

    def raw_score(c):
        key_copy(c).wait()
        if c + 1 < chunks:
            value_copy(c + 1).start()
        return dot_t(q_wide, both(keys, c))

    def soften(c, raw):
        score = raw * inv_root + latest - cumlog[:, c * chunk : (c + 1) * chunk]
        score = jnp.where(place + c * chunk < length, score, -jnp.inf)
        top = jnp.maximum(own_score, jnp.max(score, axis=1, keepdims=True))
        weight = jnp.exp(score - top)
        return top, jnp.sum(weight, axis=1, keepdims=True), weight.astype(bf16)

    soft = []
    with jax.named_scope("score"):
        raw = raw_score(0)
        cumlog_copy.wait()
        position = lax.broadcasted_iota(jnp.int32, (heads, span), 1)
        latest = (
            jnp.sum(jnp.where(position == length - 1, cumlog[...], 0.0), axis=1, keepdims=True)
            + log_gate
        )
        for c in range(1, chunks):
            following = raw_score(c)
            soft.append(soften(c - 1, raw))
            raw = following
        for copy in smalls[5:]:
            copy.start()
        out_w_copy.start()
    with jax.named_scope("av"):
        parts = []
        later = [[] for _ in range(chunks)]
        later[-1] = shared_copies + gate_up_copies + [down_copy, sdown_copy]
        for c in range(chunks):
            value_copy(c).wait()
            for copy in later[c]:
                copy.start()
            if c == chunks - 1:
                soft.append(soften(c, raw))
            parts.append(jnp.dot(soft[c][2], both(values, c), preferred_element_type=f32))
        top = own_score
        for chunk_top, _, _ in soft:
            top = jnp.maximum(top, chunk_top)
        own_weight = jnp.exp(own_score - top)
        denominator = own_weight
        weighted = jnp.zeros((heads, key_heads * head_size), f32)
        for (chunk_top, total, _), part in zip(soft, parts):
            scale = jnp.exp(chunk_top - top)
            denominator = denominator + scale * total
            weighted = weighted + scale * part
        mine = weighted[:, :head_size]
        for k in range(1, key_heads):
            mine = jnp.where(
                head_row // groups == k, weighted[:, k * head_size : (k + 1) * head_size], mine
            )
        numerator = mine + own_weight.astype(bf16).astype(f32) * own_value
        att_buf[me] = (numerator / denominator).astype(bf16)

    with jax.named_scope("barsend0"):
        pl.semaphore_wait(barrier, n - 1)
        spread(0, att_buf, recv_sem.at[0], '')

    with jax.named_scope("prep"):
        for copy in smalls[5:]:
            copy.wait()
        route_scores = route_scores_ref[...]
        gate_weights = (
            route_scores / jnp.sum(route_scores, axis=0, keepdims=True) * routed_scale
        )
        expert_row = lax.broadcasted_iota(jnp.int32, (n, rows), 0)
        share = jnp.zeros((n, rows), f32)
        for k in range(routes_ref.shape[0]):
            share = share + jnp.where(
                routes_ref[k : k + 1] == expert_row, gate_weights[k : k + 1], 0.0
            )
        row_eye = lax.broadcasted_iota(jnp.int32, (rows, rows), 0) == lax.broadcasted_iota(
            jnp.int32, (rows, rows), 1
        )
        shares = [
            jnp.sum(jnp.where(row_eye, share[e : e + 1], 0.0), axis=1, keepdims=True)
            for e in range(n)
        ]
        out_w_copy.wait()

    with jax.named_scope("arrive0"):
        arrive(0, att_buf, recv_sem.at[0], 0, n - 1)
    with jax.named_scope("oproj_send1"):
        att_wide[...] = att_buf[...].astype(f32).reshape(n * heads, head_size)
        attended = jnp.concatenate(
            [att_wide[pl.ds(h, n, stride=heads), :].astype(bf16) for h in range(heads)], axis=1
        )
        mixed = jnp.dot(attended, out_w[...], preferred_element_type=f32)
        stream = (residual_ref[...].astype(f32) + mixed).astype(bf16)
        stream_buf[me] = widen(stream)
        spread(1, stream_buf, stream_sem.at[home], 'desc')

    with jax.named_scope("wwait"):
        pltpu.make_async_copy(shared_w, shared_w, load_sem.at[2]).wait()
        pltpu.make_async_copy(gate_up_w, gate_up_w, load_sem.at[3]).wait()

    with jax.named_scope("gateup_send2"):
        weights = (shared_w.at[0], shared_w.at[1], gate_up_w.at[0], gate_up_w.at[1])
        sums = [jnp.zeros((rows, w.shape[0]), f32) for w in weights]
        squares = jnp.zeros((rows, 1), f32)
        for i in range(turns):
            c = visit(i)
            part = pl.ds(pl.multiple_of(c * wide, wide), wide)
            with jax.named_scope("w%d" % i):
                if i:
                    arrive(1, stream_buf, stream_sem.at[c], c * per, per)
                else:
                    arrive(1, stream_buf, stream_sem.at[c], 0, per - 1)
            block = join_lanes([stream_buf[c * per + t] for t in range(per)], width).astype(f32)
            squares = squares + jnp.sum(block * block, axis=1, keepdims=True)
            scaled = (block * gain_ref[:, part]).astype(bf16)
            sums = [total + dot_t(scaled, w[:, part]) for total, w in zip(sums, weights)]
        inv_rms = lax.rsqrt(squares * (1.0 / model) + norm_eps)
        sgated, supped, gated, upped = [total * inv_rms for total in sums]

        mid_buf[me] = widen((jax.nn.silu(sgated) * supped).astype(bf16))
        spread(2, mid_buf, recv_sem.at[1], 'asc')
        hidden = (jax.nn.silu(gated) * upped).astype(bf16)
    with jax.named_scope("down_send3"):
        down_copy.wait()

        def expert_out(i):
            part = pl.ds(i * wide, wide)
            return jnp.dot(hidden, down_w[:, part], preferred_element_type=f32).astype(bf16)

        def send_block(peer):
            remote(3, eo_src.at[peer], eo_buf.at[me], peer, recv_sem.at[2]).start()

        def put(c, out):
            for s in range(per):
                eo_src[c * per + s] = widen(out[:, s * width : (s + 1) * width])
            for s in range(per):
                peer = c * per + s
                pl.when(peer != me)(functools.partial(send_block, peer))

        out = expert_out(0)
        for i in range(1, turns):
            following = expert_out(i)
            put(i - 1, out)
            out = following
        put(turns - 1, out)
        eo_buf[me] = eo_src[me]

    with jax.named_scope("sentwait"):
        sdown_copy.wait()
        sent(0, att_buf)
        sent(1, stream_buf)
        sent(2, mid_buf)
    with jax.named_scope("arrive2"):
        arrive(2, mid_buf, recv_sem.at[1], 0, n - 1)
    with jax.named_scope("sdown"):
        mid = join_lanes([mid_buf[j] for j in range(n)], shared_width)
        total = stream.astype(f32) + jnp.dot(mid, sdown_w[...], preferred_element_type=f32)
    with jax.named_scope("arrive3"):
        sent(3, eo_src)
        arrive(3, eo_buf, recv_sem.at[2], 0, n - 1)
    with jax.named_scope("final"):
        for e in range(n):
            total = total + shares[e] * eo_buf[e][:, :width].astype(f32)
        out_ref[...] = total.astype(bf16)


def solution(mesh):
    n = mesh.shape["ep"]

    def on_device(
        queries,
        fresh_token_key,
        value_new,
        forget_logit,
        cache_keys,
        cache_values,
        cache_cumlog,
        lengths,
        residual,
        out_weight,
        norm_gain,
        expert_gate,
        expert_up,
        expert_down,
        shared_gate,
        shared_up,
        shared_down,
        routes,
        route_scores,
    ):
        rows, width = residual.shape
        heads, head_size = queries.shape[1:]
        span = cache_keys.shape[2]
        model = norm_gain.shape[0]
        lanes = -(-width // LANES) * LANES
        mid_lanes = -(-shared_gate.shape[0] // LANES) * LANES
        turns = model // max(width, 2 * LANES)
        chunks = 2
        hbm = pl.BlockSpec(memory_space=pltpu.HBM)

        def like(a, drop=0):
            return pltpu.VMEM(a.shape[drop:], a.dtype)

        def held(a):
            return pltpu.with_memory_space_constraint(a, pltpu.HBM)

        return pl.pallas_call(
            functools.partial(layer, n),
            out_shape=pltpu.VMEM((rows, width), bf16),
            in_specs=[pl.BlockSpec(memory_space=pl.ANY)] + [hbm] * 18,
            out_specs=pl.BlockSpec(memory_space=pltpu.VMEM),
            scratch_shapes=[
                pltpu.SMEM((1, 1), jnp.int32),
                like(queries),
                like(fresh_token_key),
                like(value_new),
                like(forget_logit),
                like(residual),
                pltpu.VMEM((1, model), f32),
                pltpu.VMEM(routes.shape[::-1], routes.dtype),
                pltpu.VMEM(route_scores.shape[::-1], f32),
                like(cache_keys, 1),
                like(cache_values, 1),
                like(cache_cumlog, 1),
                like(out_weight),
                pltpu.VMEM((2, *expert_gate.shape[1:]), bf16),
                like(expert_down, 1),
                pltpu.VMEM((2, *shared_gate.shape), bf16),
                like(shared_down),
                pltpu.VMEM((n, heads, head_size), bf16),
                pltpu.VMEM((n * heads, head_size), f32),
                pltpu.VMEM((n, rows, lanes), bf16),
                pltpu.VMEM((n, rows, mid_lanes), bf16),
                pltpu.VMEM((n, rows, lanes), bf16),
                pltpu.VMEM((n, rows, lanes), bf16),
                pltpu.SemaphoreType.DMA((9,)),
                pltpu.SemaphoreType.DMA((6,)),
                pltpu.SemaphoreType.DMA((chunks,)),
                pltpu.SemaphoreType.DMA((chunks,)),
                pltpu.SemaphoreType.DMA((4,)),
                pltpu.SemaphoreType.DMA((3,)),
                pltpu.SemaphoreType.DMA((turns,)),
            ],
            compiler_params=pltpu.CompilerParams(
                collective_id=0, has_side_effects=True, vmem_limit_bytes=VMEM_LIMIT
            ),
            name="layer",
        )(
            lengths.reshape(1, 1),
            *map(
                held,
                (
                    queries,
                    fresh_token_key,
                    value_new,
                    forget_logit,
                    residual,
                    norm_gain.reshape(1, -1),
                    routes.T,
                    route_scores.T,
                    cache_keys,
                    cache_values,
                    cache_cumlog,
                    out_weight,
                    expert_gate,
                    expert_up,
                    expert_down,
                    shared_gate,
                    shared_up,
                    shared_down,
                ),
            ),
        )

    placed = (
        P(("grp", "ep"), None, None),
        P(("grp", "ep"), None, None),
        P(("grp", "ep"), None, None),
        P(("grp", "ep"), None),
        P(("grp", "ep"), None, None, None),
        P(("grp", "ep"), None, None, None),
        P(("grp", "ep"), None, None),
        P(("grp", "ep")),
        P("grp", "ep"),
        P(None, "ep"),
        P(),
        P("ep", None, None),
        P("ep", None, None),
        P("ep", None, None),
        P("ep", None),
        P("ep", None),
        P(None, "ep"),
        P("grp", None),
        P("grp", None),
    )
    return jax.shard_map(
        on_device, mesh=mesh, in_specs=placed, out_specs=P("grp", "ep"), check_vma=False
    )
```

```python
import functools

import jax
import jax.numpy as jnp
from jax import lax
from jax.experimental import pallas as pl
from jax.experimental.pallas import tpu as pltpu
from jax.sharding import PartitionSpec as P

norm_eps = 1e-06
routed_scale = 2.5
contract_last = (((1,), (1,)), ((), ()))
LANES = 128
VMEM_LIMIT = 48 * 1024 * 1024
f32 = jnp.float32
bf16 = jnp.bfloat16


def dot_t(a, b):
    return lax.dot_general(a, b, contract_last, preferred_element_type=f32)


def join_lanes(blocks, width):
    if width % LANES == 0:
        return jnp.concatenate([b.astype(bf16) for b in blocks], axis=1)
    rows = blocks[0].shape[0]
    total = len(blocks) * width
    lane = lax.broadcasted_iota(jnp.int32, (rows, LANES), 1)
    pieces = [jnp.zeros((rows, LANES), f32) for _ in range(-(-total // LANES))]
    for k, block in enumerate(blocks):
        at, shift = divmod(k * width, LANES)
        moved = jnp.where(lane < width, block.astype(f32), 0.0)
        if shift:
            moved = pltpu.roll(moved, shift, 1)
        if shift + width <= LANES:
            pieces[at] = pieces[at] + moved
        else:
            pieces[at] = pieces[at] + jnp.where(lane >= shift, moved, 0.0)
            pieces[at + 1] = pieces[at + 1] + jnp.where(lane < shift, moved, 0.0)
    return jnp.concatenate([p.astype(bf16) for p in pieces], axis=1)[:, :total]


def widen(block):
    rows, width = block.shape
    short = -width % LANES
    if not short:
        return block
    return jnp.concatenate([block, jnp.zeros((rows, short), block.dtype)], axis=1)


def order_of(home, turns):
    sides = 2 - turns % 2
    row, side = divmod(home, sides)

    def late(c):
        other_row, other_side = divmod(c, sides)
        return (c != home, 0.55 * abs(other_row - row) + 0.6 * (other_side != side) - 0.2 * other_row)

    return sorted(range(turns), key=late)


def layer(
    n,
    lengths_hbm,
    q_hbm,
    fresh_hbm,
    vnew_hbm,
    forget_hbm,
    residual_hbm,
    gain_hbm,
    routes_hbm,
    route_scores_hbm,
    keys_hbm,
    values_hbm,
    cumlog_hbm,
    out_w_hbm,
    gate_hbm,
    up_hbm,
    down_hbm,
    sgate_hbm,
    sup_hbm,
    sdown_hbm,
    out_ref,
    lengths_ref,
    q_ref,
    fresh_ref,
    vnew_ref,
    forget_ref,
    residual_ref,
    gain_ref,
    routes_ref,
    route_scores_ref,
    keys,
    values,
    cumlog,
    out_w,
    gate_up_w,
    down_w,
    shared_w,
    sdown_w,
    att_buf,
    att_wide,
    stream_buf,
    mid_buf,
    eo_src,
    eo_buf,
    small_sem,
    load_sem,
    key_sem,
    value_sem,
    send_sem,
    recv_sem,
    stream_sem,
):
    me = lax.axis_index("ep")
    heads, head_size = q_ref.shape[1:]
    key_heads, span = keys.shape[:2]
    groups = heads // key_heads
    rows, width = residual_ref.shape
    ff, model = gate_up_w.shape[1:]
    shared_width = shared_w.shape[1]
    chunks = key_sem.shape[0]
    chunk = span // chunks

    def key_copy(c):
        part = pl.ds(c * chunk, chunk)
        return pltpu.make_async_copy(keys_hbm.at[0, :, part], keys.at[:, part], key_sem.at[c])

    value_parts = value_sem.shape[0]
    late_values = 1
    value_chunk = span // value_parts

    def value_copy(c):
        part = pl.ds(c * value_chunk, value_chunk)
        return pltpu.make_async_copy(values_hbm.at[0, :, part], values.at[:, part], value_sem.at[c])

    cumlog_copy = pltpu.make_async_copy(cumlog_hbm.at[0], cumlog, load_sem.at[0])
    out_w_copy = pltpu.make_async_copy(out_w_hbm, out_w, load_sem.at[1])
    down_copy = pltpu.make_async_copy(down_hbm.at[0], down_w, load_sem.at[4])
    sdown_copy = pltpu.make_async_copy(
        sdown_hbm, sdown_w.at[:, pl.ds(0, sdown_hbm.shape[1])], load_sem.at[5]
    )

    def pair_copies(first, second, both, sem):
        return [
            pltpu.make_async_copy(src, both.at[k], sem) for k, src in enumerate((first, second))
        ]

    shared_copies = pair_copies(sgate_hbm, sup_hbm, shared_w, load_sem.at[2])
    gate_up_copies = pair_copies(gate_hbm.at[0], up_hbm.at[0], gate_up_w, load_sem.at[3])

    smalls = [
        pltpu.make_async_copy(src, dst, small_sem.at[i])
        for i, (src, dst) in enumerate(
            (
                (q_hbm, q_ref),
                (fresh_hbm, fresh_ref),
                (vnew_hbm, vnew_ref),
                (forget_hbm, forget_ref),
                (lengths_hbm, lengths_ref),
                (routes_hbm, routes_ref),
                (route_scores_hbm, route_scores_ref),
                (residual_hbm, residual_ref),
                (gain_hbm, gain_ref),
            )
        )
    ]
    for copy in smalls[:5]:
        copy.start()
    cumlog_copy.start()
    for c in range(chunks):
        key_copy(c).start()
    for c in range(value_parts - late_values):
        value_copy(c).start()

    sdown_w[...] = jnp.zeros_like(sdown_w)
    barrier = pltpu.get_barrier_semaphore()

    def greet(i, carry):
        pl.semaphore_signal(barrier, inc=1, device_id={"ep": lax.rem(me + i, n)})
        return carry

    with jax.named_scope("greet"):
        lax.fori_loop(1, n, greet, 0)

    wide = max(width, 2 * LANES)
    per = wide // width
    turns = model // wide
    home = me // per
    toward = 1 - 2 * (home // (turns // 2))

    def remote(phase, src, dst, peer, sem):
        return pltpu.make_async_remote_copy(
            src_ref=src,
            dst_ref=dst,
            send_sem=send_sem.at[phase],
            recv_sem=sem,
            device_id={"ep": peer},
        )

    def spread(phase, buf, sem, order=""):
        def one(i, carry):
            if order == "asc":
                peer = i - 1 + (i - 1 + n - me) // n
            elif order == "desc":
                peer = n - i - (me + i) // n
                peer = n - i - jnp.where(n - i <= me, 1, 0)
            elif order == "near":
                peer = lax.rem(me + toward * i + n, n)
            else:
                peer = lax.rem(me + toward * (n - i) + n, n)
            remote(phase, buf.at[me], buf.at[me], peer, sem).start()
            return carry

        lax.fori_loop(1, n, one, 0)

    def arrive(phase, buf, sem, first, count):
        blocks = buf.at[pl.ds(first, count)]
        remote(phase, blocks, blocks, me, sem).wait_recv()

    def sent(phase, buf):
        blocks = buf.at[pl.ds(0, n - 1)]
        remote(phase, blocks, blocks, me, recv_sem.at[0]).wait_send()

    orders = [order_of(h, turns) for h in range(turns)]

    def send_mid(peer):
        remote(2, mid_buf.at[me], mid_buf.at[me], peer, recv_sem.at[1]).start()

    def visit(i):
        place = jnp.int32(orders[0][i])
        for h in range(1, turns):
            place = jnp.where(home == h, orders[h][i], place)
        return place

    inv_root = head_size ** (-0.5)
    head_row = lax.broadcasted_iota(jnp.int32, (heads, head_size), 0)
    with jax.named_scope("smallwait"):
        smalls[0].wait()
    q = q_ref[0]
    q_wide = jnp.concatenate(
        [jnp.where(head_row // groups == k, q, jnp.zeros_like(q)) for k in range(key_heads)],
        axis=1,
    )

    def both(ref, c):
        part = slice(c * chunk, (c + 1) * chunk)
        return jnp.concatenate([ref[k, part] for k in range(key_heads)], axis=1)

    def raw_score(c):
        key_copy(c).wait()
        if c < late_values:
            value_copy(value_parts - late_values + c).start()
        return dot_t(q_wide, both(keys, c))

    def soften(c, raw):
        score = raw * inv_root + latest - cumlog[:, c * chunk : (c + 1) * chunk]
        score = jnp.where(place + c * chunk < length, score, -jnp.inf)
        top = jnp.maximum(own_score, jnp.max(score, axis=1, keepdims=True))
        weight = jnp.exp(score - top)
        return top, jnp.sum(weight, axis=1, keepdims=True), weight.astype(bf16)

    raws, soft = [], []
    with jax.named_scope("score"):
        for c in range(chunks):
            raws.append(raw_score(c))
            if c == 1:
                for copy in smalls[1:5]:
                    copy.wait()
                cumlog_copy.wait()
                length = lengths_ref[0, 0]
                fresh, vnew = fresh_ref[0].astype(f32), vnew_ref[0].astype(f32)
                own_key, own_value = fresh[0:1], vnew[0:1]
                for k in range(1, key_heads):
                    own_key = jnp.where(head_row // groups == k, fresh[k : k + 1], own_key)
                    own_value = jnp.where(head_row // groups == k, vnew[k : k + 1], own_value)
                own_score = jnp.sum(q.astype(f32) * own_key, axis=1, keepdims=True) * inv_root
                eye = lax.broadcasted_iota(jnp.int32, (heads, heads), 0) == lax.broadcasted_iota(
                    jnp.int32, (heads, heads), 1
                )
                forget = jnp.sum(jnp.where(eye, forget_ref[...], 0.0), axis=1, keepdims=True)
                log_gate = jnp.minimum(forget, 0.0) - jnp.log1p(jnp.exp(-jnp.abs(forget)))
                position = lax.broadcasted_iota(jnp.int32, (heads, span), 1)
                latest = (
                    jnp.sum(jnp.where(position == length - 1, cumlog[...], 0.0), axis=1, keepdims=True)
                    + log_gate
                )
                place = lax.broadcasted_iota(jnp.int32, (heads, chunk), 1)
            if c > 1:
                while len(soft) < c:
                    soft.append(soften(len(soft), raws[len(soft)]))
        for copy in smalls[5:]:
            copy.start()
        out_w_copy.start()
    with jax.named_scope("av"):
        parts = []
        for c in range(chunks):
            if c % (chunks // value_parts) == 0:
                value_copy(c // (chunks // value_parts)).wait()
            if c == chunks - chunks // value_parts:
                for copy in shared_copies + gate_up_copies + [down_copy, sdown_copy]:
                    copy.start()
            if c == 0:
                while len(soft) < chunks:
                    soft.append(soften(len(soft), raws[len(soft)]))
            parts.append(jnp.dot(soft[c][2], both(values, c), preferred_element_type=f32))
        top = own_score
        for chunk_top, _, _ in soft:
            top = jnp.maximum(top, chunk_top)
        own_weight = jnp.exp(own_score - top)
        denominator = own_weight
        weighted = jnp.zeros((heads, key_heads * head_size), f32)
        for (chunk_top, total, _), part in zip(soft, parts):
            scale = jnp.exp(chunk_top - top)
            denominator = denominator + scale * total
            weighted = weighted + scale * part
        mine = weighted[:, :head_size]
        for k in range(1, key_heads):
            mine = jnp.where(
                head_row // groups == k, weighted[:, k * head_size : (k + 1) * head_size], mine
            )
        numerator = mine + own_weight.astype(bf16).astype(f32) * own_value
        att_buf[me] = (numerator / denominator).astype(bf16)

    with jax.named_scope("barsend0"):
        pl.semaphore_wait(barrier, n - 1)
        spread(0, att_buf, recv_sem.at[0], '')

    with jax.named_scope("prep"):
        for copy in smalls[5:]:
            copy.wait()
        route_scores = route_scores_ref[...]
        gate_weights = (
            route_scores / jnp.sum(route_scores, axis=0, keepdims=True) * routed_scale
        )
        expert_row = lax.broadcasted_iota(jnp.int32, (n, rows), 0)
        share = jnp.zeros((n, rows), f32)
        for k in range(routes_ref.shape[0]):
            share = share + jnp.where(
                routes_ref[k : k + 1] == expert_row, gate_weights[k : k + 1], 0.0
            )
        row_eye = lax.broadcasted_iota(jnp.int32, (rows, rows), 0) == lax.broadcasted_iota(
            jnp.int32, (rows, rows), 1
        )
        shares = [
            jnp.sum(jnp.where(row_eye, share[e : e + 1], 0.0), axis=1, keepdims=True)
            for e in range(n)
        ]
        out_w_copy.wait()

    with jax.named_scope("arrive0"):
        arrive(0, att_buf, recv_sem.at[0], 0, n - 1)
    with jax.named_scope("oproj_send1"):
        att_wide[...] = att_buf[...].astype(f32).reshape(n * heads, head_size)
        attended = jnp.concatenate(
            [att_wide[pl.ds(h, n, stride=heads), :].astype(bf16) for h in range(heads)], axis=1
        )
        mixed = jnp.dot(attended, out_w[...], preferred_element_type=f32)
        stream = (residual_ref[...].astype(f32) + mixed).astype(bf16)
        stream_buf[me] = widen(stream)
        spread(1, stream_buf, stream_sem.at[home], 'desc')

    with jax.named_scope("wwait"):
        pltpu.make_async_copy(shared_w, shared_w, load_sem.at[2]).wait()
        pltpu.make_async_copy(gate_up_w, gate_up_w, load_sem.at[3]).wait()

    with jax.named_scope("gateup_send2"):
        weights = (shared_w.at[0], shared_w.at[1], gate_up_w.at[0], gate_up_w.at[1])
        sums = [jnp.zeros((rows, w.shape[0]), f32) for w in weights]
        squares = jnp.zeros((rows, 1), f32)
        for i in range(turns):
            c = visit(i)
            part = pl.ds(pl.multiple_of(c * wide, wide), wide)
            with jax.named_scope("w%d" % i):
                if i:
                    arrive(1, stream_buf, stream_sem.at[c], c * per, per)
                else:
                    arrive(1, stream_buf, stream_sem.at[c], 0, per - 1)
            block = join_lanes([stream_buf[c * per + t] for t in range(per)], width).astype(f32)
            squares = squares + jnp.sum(block * block, axis=1, keepdims=True)
            scaled = (block * gain_ref[:, part]).astype(bf16)
            sums = [total + dot_t(scaled, w[:, part]) for total, w in zip(sums, weights)]
        inv_rms = lax.rsqrt(squares * (1.0 / model) + norm_eps)
        sgated, supped, gated, upped = [total * inv_rms for total in sums]

        mid_buf[me] = widen((jax.nn.silu(sgated) * supped).astype(bf16))
        for s in range(per):
            pl.when(me != s)(functools.partial(send_mid, s))
        hidden = (jax.nn.silu(gated) * upped).astype(bf16)
    with jax.named_scope("down_send3"):
        down_copy.wait()

        def expert_out(i):
            part = pl.ds(i * wide, wide)
            return jnp.dot(hidden, down_w[:, part], preferred_element_type=f32).astype(bf16)

        def send_block(peer):
            remote(3, eo_src.at[peer], eo_buf.at[me], peer, recv_sem.at[2]).start()

        def put(c, out):
            for s in range(per):
                eo_src[c * per + s] = widen(out[:, s * width : (s + 1) * width])
            for s in range(per):
                peer = c * per + s
                pl.when(peer != me)(functools.partial(send_block, peer))
                if c:
                    pl.when(peer != me)(functools.partial(send_mid, peer))

        put(0, expert_out(0))
        out = expert_out(1)
        for i in range(2, turns):
            following = expert_out(i)
            put(i - 1, out)
            out = following
        put(turns - 1, out)
        eo_buf[me] = eo_src[me]

    with jax.named_scope("sentwait"):
        sdown_copy.wait()
        sent(0, att_buf)
        sent(1, stream_buf)
        sent(2, mid_buf)
    with jax.named_scope("arrive2"):
        arrive(2, mid_buf, recv_sem.at[1], 0, n - 1)
    with jax.named_scope("sdown"):
        mid = jnp.concatenate([mid_buf[j] for j in range(n)], axis=1)
        shared_down = sdown_w[...].reshape(mid.shape[1], width)
        total = stream.astype(f32) + jnp.dot(mid, shared_down, preferred_element_type=f32)
    with jax.named_scope("arrive3"):
        sent(3, eo_src)
        arrive(3, eo_buf, recv_sem.at[2], 0, n - 1)
    with jax.named_scope("final"):
        for e in range(n):
            total = total + shares[e] * eo_buf[e][:, :width].astype(f32)
        out_ref[...] = total.astype(bf16)


def solution(mesh):
    n = mesh.shape["ep"]

    def on_device(
        queries,
        fresh_token_key,
        value_new,
        forget_logit,
        cache_keys,
        cache_values,
        cache_cumlog,
        lengths,
        residual,
        out_weight,
        norm_gain,
        expert_gate,
        expert_up,
        expert_down,
        shared_gate,
        shared_up,
        shared_down,
        routes,
        route_scores,
    ):
        rows, width = residual.shape
        heads, head_size = queries.shape[1:]
        span = cache_keys.shape[2]
        model = norm_gain.shape[0]
        lanes = -(-width // LANES) * LANES
        mid_lanes = -(-shared_gate.shape[0] // LANES) * LANES
        turns = model // max(width, 2 * LANES)
        chunks = 4
        hbm = pl.BlockSpec(memory_space=pltpu.HBM)

        def like(a, drop=0):
            return pltpu.VMEM(a.shape[drop:], a.dtype)

        def held(a):
            return pltpu.with_memory_space_constraint(a, pltpu.HBM)

        return pl.pallas_call(
            functools.partial(layer, n),
            out_shape=pltpu.VMEM((rows, width), bf16),
            in_specs=[pl.BlockSpec(memory_space=pl.ANY)] + [hbm] * 18,
            out_specs=pl.BlockSpec(memory_space=pltpu.VMEM),
            scratch_shapes=[
                pltpu.SMEM((1, 1), jnp.int32),
                like(queries),
                like(fresh_token_key),
                like(value_new),
                like(forget_logit),
                like(residual),
                pltpu.VMEM((1, model), f32),
                pltpu.VMEM(routes.shape[::-1], routes.dtype),
                pltpu.VMEM(route_scores.shape[::-1], f32),
                like(cache_keys, 1),
                like(cache_values, 1),
                like(cache_cumlog, 1),
                like(out_weight),
                pltpu.VMEM((2, *expert_gate.shape[1:]), bf16),
                like(expert_down, 1),
                pltpu.VMEM((2, *shared_gate.shape), bf16),
                pltpu.VMEM((n, mid_lanes, width), bf16),
                pltpu.VMEM((n, heads, head_size), bf16),
                pltpu.VMEM((n * heads, head_size), f32),
                pltpu.VMEM((n, rows, lanes), bf16),
                pltpu.VMEM((n, rows, mid_lanes), bf16),
                pltpu.VMEM((n, rows, lanes), bf16),
                pltpu.VMEM((n, rows, lanes), bf16),
                pltpu.SemaphoreType.DMA((9,)),
                pltpu.SemaphoreType.DMA((6,)),
                pltpu.SemaphoreType.DMA((chunks,)),
                pltpu.SemaphoreType.DMA((2,)),
                pltpu.SemaphoreType.DMA((4,)),
                pltpu.SemaphoreType.DMA((3,)),
                pltpu.SemaphoreType.DMA((turns,)),
            ],
            compiler_params=pltpu.CompilerParams(
                collective_id=0, has_side_effects=True, vmem_limit_bytes=VMEM_LIMIT
            ),
            name="layer",
        )(
            lengths.reshape(1, 1),
            *map(
                held,
                (
                    queries,
                    fresh_token_key,
                    value_new,
                    forget_logit,
                    residual,
                    norm_gain.reshape(1, -1),
                    routes.T,
                    route_scores.T,
                    cache_keys,
                    cache_values,
                    cache_cumlog,
                    out_weight,
                    expert_gate,
                    expert_up,
                    expert_down,
                    shared_gate,
                    shared_up,
                    shared_down.reshape(n, -1, width),
                ),
            ),
        )

    placed = (
        P(("grp", "ep"), None, None),
        P(("grp", "ep"), None, None),
        P(("grp", "ep"), None, None),
        P(("grp", "ep"), None),
        P(("grp", "ep"), None, None, None),
        P(("grp", "ep"), None, None, None),
        P(("grp", "ep"), None, None),
        P(("grp", "ep")),
        P("grp", "ep"),
        P(None, "ep"),
        P(),
        P("ep", None, None),
        P("ep", None, None),
        P("ep", None, None),
        P("ep", None),
        P("ep", None),
        P(None, "ep"),
        P("grp", None),
        P("grp", None),
    )
    return jax.shard_map(
        on_device, mesh=mesh, in_specs=placed, out_specs=P("grp", "ep"), check_vma=False
    )
```

```python
import functools

import jax
import jax.numpy as jnp
from jax import lax
from jax.experimental import pallas as pl
from jax.experimental.pallas import tpu as pltpu
from jax.sharding import PartitionSpec as P

norm_eps = 1e-06
routed_scale = 2.5
contract_last = (((1,), (1,)), ((), ()))
LANES = 128
VMEM_LIMIT = 48 * 1024 * 1024
f32 = jnp.float32
bf16 = jnp.bfloat16


def dot_t(a, b):
    return lax.dot_general(a, b, contract_last, preferred_element_type=f32)


def join_lanes(blocks, width):
    if width % LANES == 0:
        return jnp.concatenate([b.astype(bf16) for b in blocks], axis=1)
    rows = blocks[0].shape[0]
    total = len(blocks) * width
    lane = lax.broadcasted_iota(jnp.int32, (rows, LANES), 1)
    pieces = [jnp.zeros((rows, LANES), f32) for _ in range(-(-total // LANES))]
    for k, block in enumerate(blocks):
        at, shift = divmod(k * width, LANES)
        moved = jnp.where(lane < width, block.astype(f32), 0.0)
        if shift:
            moved = pltpu.roll(moved, shift, 1)
        if shift + width <= LANES:
            pieces[at] = pieces[at] + moved
        else:
            pieces[at] = pieces[at] + jnp.where(lane >= shift, moved, 0.0)
            pieces[at + 1] = pieces[at + 1] + jnp.where(lane < shift, moved, 0.0)
    return jnp.concatenate([p.astype(bf16) for p in pieces], axis=1)[:, :total]


def widen(block):
    rows, width = block.shape
    short = -width % LANES
    if not short:
        return block
    return jnp.concatenate([block, jnp.zeros((rows, short), block.dtype)], axis=1)


def order_of(home, turns):
    sides = 2 - turns % 2
    row, side = divmod(home, sides)

    def late(c):
        other_row, other_side = divmod(c, sides)
        return (c != home, 0.55 * abs(other_row - row) + 0.6 * (other_side != side) - 0.2 * other_row)

    return sorted(range(turns), key=late)


def layer(
    n,
    lengths_hbm,
    q_hbm,
    fresh_hbm,
    vnew_hbm,
    forget_hbm,
    residual_hbm,
    gain_hbm,
    routes_hbm,
    route_scores_hbm,
    keys_hbm,
    values_hbm,
    cumlog_hbm,
    out_w_hbm,
    gate_hbm,
    up_hbm,
    down_hbm,
    sgate_hbm,
    sup_hbm,
    sdown_hbm,
    out_ref,
    lengths_ref,
    q_ref,
    fresh_ref,
    vnew_ref,
    forget_ref,
    residual_ref,
    gain_ref,
    routes_ref,
    route_scores_ref,
    keys,
    values,
    cumlog,
    out_w,
    gate_up_w,
    down_w,
    shared_w,
    sdown_w,
    att_buf,
    att_wide,
    stream_buf,
    mid_buf,
    eo_src,
    eo_buf,
    small_sem,
    load_sem,
    key_sem,
    value_sem,
    send_sem,
    recv_sem,
    stream_sem,
):
    me = lax.axis_index("ep")
    heads, head_size = q_ref.shape[1:]
    key_heads, span = keys.shape[:2]
    groups = heads // key_heads
    rows, width = residual_ref.shape[1:]
    ff, model = gate_up_w.shape[1:]
    shared_width = shared_w.shape[1]
    chunks = key_sem.shape[0]
    chunk = span // chunks

    def key_copy(c):
        part = pl.ds(c * chunk, chunk)
        return pltpu.make_async_copy(keys_hbm.at[0, :, part], keys.at[:, part], key_sem.at[c])

    value_parts = value_sem.shape[0]
    late_values = 1
    value_chunk = span // value_parts

    def value_copy(c):
        part = pl.ds(c * value_chunk, value_chunk)
        return pltpu.make_async_copy(values_hbm.at[0, :, part], values.at[:, part], value_sem.at[c])

    cumlog_copy = pltpu.make_async_copy(cumlog_hbm.at[0], cumlog, load_sem.at[0])
    out_w_copy = pltpu.make_async_copy(
        out_w_hbm, out_w.at[lax.rem(me, 2)], load_sem.at[1]
    )
    down_copy = pltpu.make_async_copy(down_hbm.at[0], down_w, load_sem.at[4])
    sdown_copy = pltpu.make_async_copy(
        sdown_hbm, sdown_w.at[:, pl.ds(0, sdown_hbm.shape[1])], load_sem.at[5]
    )

    def pair_copies(first, second, both, sem):
        return [
            pltpu.make_async_copy(src, both.at[k], sem) for k, src in enumerate((first, second))
        ]

    shared_copies = pair_copies(sgate_hbm, sup_hbm, shared_w, load_sem.at[2])
    gate_up_copies = pair_copies(gate_hbm.at[0], up_hbm.at[0], gate_up_w, load_sem.at[3])

    smalls = [
        pltpu.make_async_copy(src, dst, small_sem.at[i])
        for i, (src, dst) in enumerate(
            (
                (q_hbm, q_ref),
                (fresh_hbm, fresh_ref),
                (vnew_hbm, vnew_ref),
                (forget_hbm, forget_ref),
                (lengths_hbm, lengths_ref),
                (routes_hbm, routes_ref),
                (route_scores_hbm, route_scores_ref),
                (residual_hbm, residual_ref.at[lax.rem(me, 2)]),
                (gain_hbm, gain_ref),
            )
        )
    ]
    key_copy(0).start()
    for copy in smalls[:5]:
        copy.start()
    cumlog_copy.start()
    for c in range(1, chunks):
        key_copy(c).start()
    for c in range(value_parts - late_values):
        value_copy(c).start()
    sdown_w[...] = jnp.zeros_like(sdown_w)
    barrier = pltpu.get_barrier_semaphore()

    with jax.named_scope("greet"):
        for i in range(1, n):
            pl.semaphore_signal(barrier, inc=1, device_id={"ep": lax.rem(me + i, n)})

    wide = 2 * max(width, LANES)
    per = wide // width
    pairs, pair_per = n // 2, per // 2
    pair, side = me // 2, lax.rem(me, 2)
    leads = side == 1
    turns = model // wide
    home = me // per
    toward = 1 - 2 * (home // (turns // 2))

    def remote(phase, src, dst, peer, sem):
        return pltpu.make_async_remote_copy(
            src_ref=src,
            dst_ref=dst,
            send_sem=send_sem.at[phase],
            recv_sem=sem,
            device_id={"ep": peer},
        )

    def arrive(phase, buf, sem, first, count):
        blocks = buf.at[pl.ds(first, count)]
        remote(phase, blocks, blocks, me, sem).wait_recv()

    def sent(phase, buf, count):
        blocks = buf.at[pl.ds(0, count)]
        remote(phase, blocks, blocks, me, recv_sem.at[0]).wait_send()

    orders = [order_of(h, turns) for h in range(turns)]

    def send_mid(peer):
        remote(5, mid_buf.at[me], mid_buf.at[me], peer, recv_sem.at[1]).start()

    def visit(i):
        place = jnp.int32(orders[0][i])
        for h in range(1, turns):
            place = jnp.where(home == h, orders[h][i], place)
        return place

    inv_root = head_size ** (-0.5)
    head_row = lax.broadcasted_iota(jnp.int32, (heads, head_size), 0)
    with jax.named_scope("smallwait"):
        smalls[0].wait()
    q = q_ref[0]
    q_wide = jnp.concatenate(
        [jnp.where(head_row // groups == k, q, jnp.zeros_like(q)) for k in range(key_heads)],
        axis=1,
    )

    def both(ref, c):
        part = slice(c * chunk, (c + 1) * chunk)
        return jnp.concatenate([ref[k, part] for k in range(key_heads)], axis=1)

    def raw_score(c):
        key_copy(c).wait()
        if c < late_values:
            value_copy(value_parts - late_values + c).start()
        return dot_t(q_wide, both(keys, c))

    def soften(c, raw):
        score = raw * inv_root + latest - cumlog[:, c * chunk : (c + 1) * chunk]
        score = jnp.where(place + c * chunk < length, score, -jnp.inf)
        top = jnp.maximum(own_score, jnp.max(score, axis=1, keepdims=True))
        weight = jnp.exp(score - top)
        return top, jnp.sum(weight, axis=1, keepdims=True), weight.astype(bf16)

    raws, soft = [], []
    with jax.named_scope("score"):
        for c in range(chunks):
            raws.append(raw_score(c))
            if c == 1:
                for copy in smalls[1:5]:
                    copy.wait()
                cumlog_copy.wait()
                length = lengths_ref[0, 0]
                fresh, vnew = fresh_ref[0].astype(f32), vnew_ref[0].astype(f32)
                own_key, own_value = fresh[0:1], vnew[0:1]
                for k in range(1, key_heads):
                    own_key = jnp.where(head_row // groups == k, fresh[k : k + 1], own_key)
                    own_value = jnp.where(head_row // groups == k, vnew[k : k + 1], own_value)
                own_score = jnp.sum(q.astype(f32) * own_key, axis=1, keepdims=True) * inv_root
                eye = lax.broadcasted_iota(jnp.int32, (heads, heads), 0) == lax.broadcasted_iota(
                    jnp.int32, (heads, heads), 1
                )
                forget = jnp.sum(jnp.where(eye, forget_ref[...], 0.0), axis=1, keepdims=True)
                log_gate = jnp.minimum(forget, 0.0) - jnp.log1p(jnp.exp(-jnp.abs(forget)))
                position = lax.broadcasted_iota(jnp.int32, (heads, span), 1)
                latest = (
                    jnp.sum(jnp.where(position == length - 1, cumlog[...], 0.0), axis=1, keepdims=True)
                    + log_gate
                )
                place = lax.broadcasted_iota(jnp.int32, (heads, chunk), 1)
            if c > 1:
                while len(soft) < c:
                    soft.append(soften(len(soft), raws[len(soft)]))
        for copy in smalls[5:]:
            copy.start()
        out_w_copy.start()
    with jax.named_scope("av"):
        parts = []
        for c in range(chunks):
            if c % (chunks // value_parts) == 0:
                value_copy(c // (chunks // value_parts)).wait()
            if c == 0:
                while len(soft) < chunks:
                    soft.append(soften(len(soft), raws[len(soft)]))
            parts.append(jnp.dot(soft[c][2], both(values, c), preferred_element_type=f32))
        top = own_score
        for chunk_top, _, _ in soft:
            top = jnp.maximum(top, chunk_top)
        own_weight = jnp.exp(own_score - top)
        denominator = own_weight
        weighted = jnp.zeros((heads, key_heads * head_size), f32)
        for (chunk_top, total, _), part in zip(soft, parts):
            scale = jnp.exp(chunk_top - top)
            denominator = denominator + scale * total
            weighted = weighted + scale * part
        mine = weighted[:, :head_size]
        for k in range(1, key_heads):
            mine = jnp.where(
                head_row // groups == k, weighted[:, k * head_size : (k + 1) * head_size], mine
            )
        numerator = mine + own_weight.astype(bf16).astype(f32) * own_value
        att_buf[me] = (numerator / denominator).astype(bf16)

    with jax.named_scope("barsend0"):
        pl.semaphore_wait(barrier, n - 1)
        def send_row(to):
            peer = 2 * to + 1
            remote(0, att_buf.at[me], att_buf.at[me], peer, recv_sem.at[0]).start()

        outward = 1 - 2 * (pair // (pairs // 2))
        for i in range(1, pairs):
            send_row(lax.rem(pair + outward * (pairs - i) + pairs, pairs))
        pl.when(side == 0)(functools.partial(send_row, pair))
        for copy in shared_copies + gate_up_copies + [down_copy, sdown_copy]:
            copy.start()

    def lend(phase, buf, sem):
        return remote(phase, buf.at[0], buf.at[0], me + 1 - 2 * side, sem)

    lent = (lend(3, out_w, recv_sem.at[3]), lend(4, residual_ref, recv_sem.at[4]))
    with jax.named_scope("lend"):
        for copy in smalls[5:]:
            copy.wait()
        out_w_copy.wait()

        @pl.when(side == 0)
        def _():
            for copy in lent:
                copy.start()

    with jax.named_scope("prep"):
        route_scores = route_scores_ref[...]
        gate_weights = (
            route_scores / jnp.sum(route_scores, axis=0, keepdims=True) * routed_scale
        )
        expert_row = lax.broadcasted_iota(jnp.int32, (n, rows), 0)
        share = jnp.zeros((n, rows), f32)
        for k in range(routes_ref.shape[0]):
            share = share + jnp.where(
                routes_ref[k : k + 1] == expert_row, gate_weights[k : k + 1], 0.0
            )
        row_eye = lax.broadcasted_iota(jnp.int32, (rows, rows), 0) == lax.broadcasted_iota(
            jnp.int32, (rows, rows), 1
        )
        shares = [
            jnp.sum(jnp.where(row_eye, share[e : e + 1], 0.0), axis=1, keepdims=True)
            for e in range(n)
        ]

    def project():
        for copy in lent:
            copy.wait_recv()
        with jax.named_scope("arrive0"):
            arrive(0, att_buf, recv_sem.at[0], 0, n - 1)
        with jax.named_scope("oproj_send1"):
            att_wide[...] = att_buf[...].astype(f32).reshape(n * heads, head_size)
            attended = jnp.concatenate(
                [att_wide[pl.ds(h, n, stride=heads), :].astype(bf16) for h in range(heads)], axis=1
            )
            halves = []
            for k in range(2):
                mixed = jnp.dot(attended, out_w[k], preferred_element_type=f32)
                halves.append(widen((residual_ref[k].astype(f32) + mixed).astype(bf16)))
            stream_buf[pair] = widen(join_lanes(halves, width))
            for i in range(1, n):
                peer = n - i - jnp.where(n - i <= me, 1, 0)
                block = stream_buf.at[pair]
                remote(1 + lax.rem(peer, 2), block, block, peer, stream_sem.at[home]).start()

    pl.when(leads)(project)

    with jax.named_scope("wwait"):
        pltpu.make_async_copy(shared_w, shared_w, load_sem.at[2]).wait()
        pltpu.make_async_copy(gate_up_w, gate_up_w, load_sem.at[3]).wait()

    with jax.named_scope("gateup_send2"):
        weights = (shared_w.at[0], shared_w.at[1], gate_up_w.at[0], gate_up_w.at[1])
        sums = [jnp.zeros((rows, w.shape[0]), f32) for w in weights]
        squares = jnp.zeros((rows, 1), f32)
        for i in range(turns):
            c = visit(i)
            part = pl.ds(pl.multiple_of(c * wide, wide), wide)
            with jax.named_scope("w%d" % i):
                come = functools.partial(arrive, 1, stream_buf, stream_sem.at[c])
                if i:
                    come(c * pair_per, pair_per)
                else:
                    pl.when(side == 0)(functools.partial(come, 0, pair_per))
                    if pair_per > 1:
                        pl.when(leads)(functools.partial(come, 0, pair_per - 1))
            block = join_lanes(
                [stream_buf[c * pair_per + t] for t in range(pair_per)], 2 * width
            ).astype(f32)
            squares = squares + jnp.sum(block * block, axis=1, keepdims=True)
            scaled = (block * gain_ref[:, part]).astype(bf16)
            sums = [total + dot_t(scaled, w[:, part]) for total, w in zip(sums, weights)]
        inv_rms = lax.rsqrt(squares * (1.0 / model) + norm_eps)
        sgated, supped, gated, upped = [total * inv_rms for total in sums]

        mid_buf[me] = widen((jax.nn.silu(sgated) * supped).astype(bf16))
        for s in range(per):
            pl.when(me != s)(functools.partial(send_mid, s))
        hidden = (jax.nn.silu(gated) * upped).astype(bf16)
    with jax.named_scope("down_send3"):
        down_copy.wait()

        def expert_out(i):
            part = pl.ds(i * wide, wide)
            return jnp.dot(hidden, down_w[:, part], preferred_element_type=f32).astype(bf16)

        def send_block(peer):
            remote(6, eo_src.at[peer], eo_buf.at[me], peer, recv_sem.at[2]).start()

        def put(c, out):
            for s in range(per):
                eo_src[c * per + s] = widen(out[:, s * width : (s + 1) * width])
            for s in range(per):
                peer = c * per + s
                pl.when(peer != me)(functools.partial(send_block, peer))
                if c:
                    pl.when(peer != me)(functools.partial(send_mid, peer))

        put(0, expert_out(0))
        out = expert_out(1)
        for i in range(2, turns):
            following = expert_out(i)
            put(i - 1, out)
            out = following
        put(turns - 1, out)
        eo_buf[me] = eo_src[me]

    with jax.named_scope("sentwait"):
        sdown_copy.wait()

        @pl.when(side == 0)
        def _():
            sent(0, att_buf, pairs)
            for copy in lent:
                copy.wait_send()

        @pl.when(leads)
        def _():
            sent(0, att_buf, pairs - 1)
            sent(1, stream_buf, pairs)
            sent(2, stream_buf, pairs - 1)

        sent(5, mid_buf, n - 1)
    with jax.named_scope("arrive2"):
        arrive(2, mid_buf, recv_sem.at[1], 0, n - 1)
    with jax.named_scope("sdown"):
        mid = jnp.concatenate([mid_buf[j] for j in range(n)], axis=1)
        shared_down = sdown_w[...].reshape(mid.shape[1], width)
        mine = stream_buf[pair].astype(f32)
        stream = jnp.where(leads, mine[:, width : 2 * width], mine[:, :width])
        total = stream + jnp.dot(mid, shared_down, preferred_element_type=f32)
    with jax.named_scope("arrive3"):
        sent(6, eo_src, n - 1)
        arrive(3, eo_buf, recv_sem.at[2], 0, n - 1)
    with jax.named_scope("final"):
        for e in range(n):
            total = total + shares[e] * eo_buf[e][:, :width].astype(f32)
        out_ref[...] = total.astype(bf16)


def solution(mesh):
    n = mesh.shape["ep"]

    def on_device(
        queries,
        fresh_token_key,
        value_new,
        forget_logit,
        cache_keys,
        cache_values,
        cache_cumlog,
        lengths,
        residual,
        out_weight,
        norm_gain,
        expert_gate,
        expert_up,
        expert_down,
        shared_gate,
        shared_up,
        shared_down,
        routes,
        route_scores,
    ):
        rows, width = residual.shape
        heads, head_size = queries.shape[1:]
        span = cache_keys.shape[2]
        model = norm_gain.shape[0]
        lanes = -(-width // LANES) * LANES
        mid_lanes = -(-shared_gate.shape[0] // LANES) * LANES
        pair_lanes = -(-2 * width // LANES) * LANES
        turns = model // (2 * max(width, LANES))
        chunks = 4
        hbm = pl.BlockSpec(memory_space=pltpu.HBM)

        def like(a, drop=0):
            return pltpu.VMEM(a.shape[drop:], a.dtype)

        def held(a):
            return pltpu.with_memory_space_constraint(a, pltpu.HBM)

        return pl.pallas_call(
            functools.partial(layer, n),
            out_shape=pltpu.VMEM((rows, width), bf16),
            in_specs=[pl.BlockSpec(memory_space=pl.ANY)] + [hbm] * 18,
            out_specs=pl.BlockSpec(memory_space=pltpu.VMEM),
            scratch_shapes=[
                pltpu.SMEM((1, 1), jnp.int32),
                like(queries),
                like(fresh_token_key),
                like(value_new),
                like(forget_logit),
                pltpu.VMEM((2, *residual.shape), bf16),
                pltpu.VMEM((1, model), f32),
                pltpu.VMEM(routes.shape[::-1], routes.dtype),
                pltpu.VMEM(route_scores.shape[::-1], f32),
                like(cache_keys, 1),
                like(cache_values, 1),
                like(cache_cumlog, 1),
                pltpu.VMEM((2, *out_weight.shape), bf16),
                pltpu.VMEM((2, *expert_gate.shape[1:]), bf16),
                like(expert_down, 1),
                pltpu.VMEM((2, *shared_gate.shape), bf16),
                pltpu.VMEM((n, mid_lanes, width), bf16),
                pltpu.VMEM((n, heads, head_size), bf16),
                pltpu.VMEM((n * heads, head_size), f32),
                pltpu.VMEM((n // 2, rows, pair_lanes), bf16),
                pltpu.VMEM((n, rows, mid_lanes), bf16),
                pltpu.VMEM((n, rows, lanes), bf16),
                pltpu.VMEM((n, rows, lanes), bf16),
                pltpu.SemaphoreType.DMA((9,)),
                pltpu.SemaphoreType.DMA((6,)),
                pltpu.SemaphoreType.DMA((chunks,)),
                pltpu.SemaphoreType.DMA((2,)),
                pltpu.SemaphoreType.DMA((7,)),
                pltpu.SemaphoreType.DMA((5,)),
                pltpu.SemaphoreType.DMA((turns,)),
            ],
            compiler_params=pltpu.CompilerParams(
                collective_id=0, has_side_effects=True, vmem_limit_bytes=VMEM_LIMIT
            ),
            name="layer",
        )(
            lengths.reshape(1, 1),
            *map(
                held,
                (
                    queries,
                    fresh_token_key,
                    value_new,
                    forget_logit,
                    residual,
                    norm_gain.reshape(1, -1),
                    routes.T,
                    route_scores.T,
                    cache_keys,
                    cache_values,
                    cache_cumlog,
                    out_weight,
                    expert_gate,
                    expert_up,
                    expert_down,
                    shared_gate,
                    shared_up,
                    shared_down.reshape(n, -1, width),
                ),
            ),
        )

    placed = (
        P(("grp", "ep"), None, None),
        P(("grp", "ep"), None, None),
        P(("grp", "ep"), None, None),
        P(("grp", "ep"), None),
        P(("grp", "ep"), None, None, None),
        P(("grp", "ep"), None, None, None),
        P(("grp", "ep"), None, None),
        P(("grp", "ep")),
        P("grp", "ep"),
        P(None, "ep"),
        P(),
        P("ep", None, None),
        P("ep", None, None),
        P("ep", None, None),
        P("ep", None),
        P("ep", None),
        P(None, "ep"),
        P("grp", None),
        P("grp", None),
    )
    return jax.shard_map(
        on_device, mesh=mesh, in_specs=placed, out_specs=P("grp", "ep"), check_vma=False
    )
```

```python
import functools

import jax
import jax.numpy as jnp
from jax import lax
from jax.experimental import pallas as pl
from jax.experimental.pallas import tpu as pltpu
from jax.sharding import PartitionSpec as P

norm_eps = 1e-06
routed_scale = 2.5
contract_last = (((1,), (1,)), ((), ()))
LANES = 128
VMEM_LIMIT = 48 * 1024 * 1024
f32 = jnp.float32
bf16 = jnp.bfloat16


def dot_t(a, b):
    return lax.dot_general(a, b, contract_last, preferred_element_type=f32)


def join_lanes(blocks, width):
    if width % LANES == 0:
        return jnp.concatenate([b.astype(bf16) for b in blocks], axis=1)
    rows = blocks[0].shape[0]
    total = len(blocks) * width
    lane = lax.broadcasted_iota(jnp.int32, (rows, LANES), 1)
    pieces = [jnp.zeros((rows, LANES), f32) for _ in range(-(-total // LANES))]
    for k, block in enumerate(blocks):
        at, shift = divmod(k * width, LANES)
        moved = jnp.where(lane < width, block.astype(f32), 0.0)
        if shift:
            moved = pltpu.roll(moved, shift, 1)
        if shift + width <= LANES:
            pieces[at] = pieces[at] + moved
        else:
            pieces[at] = pieces[at] + jnp.where(lane >= shift, moved, 0.0)
            pieces[at + 1] = pieces[at + 1] + jnp.where(lane < shift, moved, 0.0)
    return jnp.concatenate([p.astype(bf16) for p in pieces], axis=1)[:, :total]


def widen(block):
    rows, width = block.shape
    short = -width % LANES
    if not short:
        return block
    return jnp.concatenate([block, jnp.zeros((rows, short), block.dtype)], axis=1)


def hops(a, b, sides):
    return abs(a // sides - b // sides) + (a % sides != b % sides)


def visit_order(home, turns):
    sides = 2 - turns % 2

    def late(c):
        sent = max(hops(c, turns - 1, sides), hops(c, 0, sides) - 1)
        return (c != home, 0.55 * abs(c // sides - home // sides) + 0.6 * (c % sides != home % sides) - 0.2 * (c // sides))

    return sorted(range(turns), key=late)


def send_order(home, pairs):
    sides = 2 - pairs % 2
    return sorted((c for c in range(pairs) if c != home), key=lambda c: -c)


def pick(table, at):
    entry = jnp.int32(table[0])
    for h in range(1, len(table)):
        entry = jnp.where(at == h, table[h], entry)
    return entry


def layer(
    n,
    lengths_hbm,
    q_hbm,
    fresh_hbm,
    vnew_hbm,
    forget_hbm,
    residual_hbm,
    gain_hbm,
    routes_hbm,
    route_scores_hbm,
    keys_hbm,
    values_hbm,
    cumlog_hbm,
    out_w_hbm,
    gate_hbm,
    up_hbm,
    down_hbm,
    sgate_hbm,
    sup_hbm,
    sdown_hbm,
    out_ref,
    lengths_ref,
    q_ref,
    fresh_ref,
    vnew_ref,
    forget_ref,
    residual_ref,
    gain_ref,
    routes_ref,
    route_scores_ref,
    keys,
    values,
    cumlog,
    out_w,
    gate_up_w,
    down_w,
    shared_w,
    sdown_w,
    att_buf,
    att_wide,
    stream_buf,
    mid_buf,
    eo_src,
    eo_buf,
    first_shared,
    first_expert,
    small_sem,
    key_sem,
    value_sem,
    send_sem,
    recv_sem,
    stream_sem,
):
    me = lax.axis_index("ep")
    heads, head_size = q_ref.shape[1:]
    key_heads, span = keys.shape[:2]
    groups = heads // key_heads
    rows, width = residual_ref.shape[1:]
    ff, model = gate_up_w.shape[1:]
    shared_width = shared_w.shape[1]
    chunks = key_sem.shape[0]
    chunk = span // chunks

    def key_copy(c):
        part = pl.ds(c * chunk, chunk)
        return pltpu.make_async_copy(keys_hbm.at[0, :, part], keys.at[:, part], key_sem.at[c])

    value_parts = value_sem.shape[0] - 1
    late_values = 1
    value_chunk = span // value_parts

    def value_copy(c):
        part = pl.ds(c * value_chunk, value_chunk)
        return pltpu.make_async_copy(values_hbm.at[0, :, part], values.at[:, part], value_sem.at[c])

    cumlog_copy = pltpu.make_async_copy(cumlog_hbm.at[0], cumlog, value_sem.at[2])
    out_w_copy = pltpu.make_async_copy(
        out_w_hbm, out_w.at[lax.rem(me, 2)], key_sem.at[1]
    )
    down_copy = pltpu.make_async_copy(down_hbm.at[0], down_w, key_sem.at[0])
    sdown_copy = pltpu.make_async_copy(
        sdown_hbm, sdown_w.at[:, pl.ds(0, sdown_hbm.shape[1])], small_sem.at[4]
    )

    def pair_copies(first, second, both, sem):
        return [
            pltpu.make_async_copy(src, both.at[k], sem) for k, src in enumerate((first, second))
        ]

    shared_copies = pair_copies(sgate_hbm, sup_hbm, shared_w, key_sem.at[2])
    gate_up_copies = pair_copies(gate_hbm.at[0], up_hbm.at[0], gate_up_w, key_sem.at[3])

    smalls = [
        pltpu.make_async_copy(src, dst, small_sem.at[i % 5])
        for i, (src, dst) in enumerate(
            (
                (q_hbm, q_ref),
                (fresh_hbm, fresh_ref),
                (vnew_hbm, vnew_ref),
                (forget_hbm, forget_ref),
                (lengths_hbm, lengths_ref),
                (routes_hbm, routes_ref),
                (route_scores_hbm, route_scores_ref),
                (residual_hbm, residual_ref.at[lax.rem(me, 2)]),
                (gain_hbm, gain_ref),
            )
        )
    ]
    key_copy(0).start()
    for copy in smalls[:5]:
        copy.start()
    cumlog_copy.start()
    for c in range(1, chunks):
        key_copy(c).start()
    for c in range(value_parts - late_values):
        value_copy(c).start()
    sdown_w[...] = jnp.zeros_like(sdown_w)
    barrier = pltpu.get_barrier_semaphore()

    with jax.named_scope("greet"):
        for i in range(1, n):
            pl.semaphore_signal(barrier, inc=1, device_id={"ep": lax.rem(me + i, n)})

    wide = 2 * max(width, LANES)
    per = wide // width
    pairs, pair_per = n // 2, per // 2
    pair, side = me // 2, lax.rem(me, 2)
    leads = side == 1
    turns = model // wide
    home = me // per
    toward = 1 - 2 * (home // (turns // 2))

    def remote(phase, src, dst, peer, sem):
        return pltpu.make_async_remote_copy(
            src_ref=src,
            dst_ref=dst,
            send_sem=send_sem.at[phase],
            recv_sem=sem,
            device_id={"ep": peer},
        )

    def arrive(phase, buf, sem, first, count):
        blocks = buf.at[pl.ds(first, count)]
        remote(phase, blocks, blocks, me, sem).wait_recv()

    def sent(phase, buf, count):
        blocks = buf.at[pl.ds(0, count)]
        remote(phase, blocks, blocks, me, recv_sem.at[0]).wait_send()

    visits = [visit_order(h, turns) for h in range(turns)]
    targets = [send_order(h, pairs) for h in range(pairs)]

    def visit(i):
        return pick([order[i] for order in visits], home)

    def send_mid(k):
        peer = k + jnp.where(me <= k, 1, 0)
        remote(0, mid_buf.at[me], mid_buf.at[me], peer, recv_sem.at[0]).start()

    inv_root = head_size ** (-0.5)
    head_row = lax.broadcasted_iota(jnp.int32, (heads, head_size), 0)
    with jax.named_scope("smallwait"):
        smalls[0].wait()
    q = q_ref[0]
    q_wide = jnp.concatenate(
        [jnp.where(head_row // groups == k, q, jnp.zeros_like(q)) for k in range(key_heads)],
        axis=1,
    )

    def both(ref, c):
        part = slice(c * chunk, (c + 1) * chunk)
        return jnp.concatenate([ref[k, part] for k in range(key_heads)], axis=1)

    def raw_score(c):
        key_copy(c).wait()
        if c < late_values:
            value_copy(value_parts - late_values + c).start()
        return dot_t(q_wide, both(keys, c))

    def soften(c, raw):
        score = raw * inv_root + latest - cumlog[:, c * chunk : (c + 1) * chunk]
        score = jnp.where(place + c * chunk < length, score, -jnp.inf)
        top = jnp.maximum(own_score, jnp.max(score, axis=1, keepdims=True))
        weight = jnp.exp(score - top)
        return top, jnp.sum(weight, axis=1, keepdims=True), weight.astype(bf16)

    raws, soft = [], []
    with jax.named_scope("score"):
        for c in range(chunks):
            raws.append(raw_score(c))
            if c == 1:
                for copy in smalls[1:5]:
                    copy.wait()
                cumlog_copy.wait()
                length = lengths_ref[0, 0]
                fresh, vnew = fresh_ref[0].astype(f32), vnew_ref[0].astype(f32)
                own_key, own_value = fresh[0:1], vnew[0:1]
                for k in range(1, key_heads):
                    own_key = jnp.where(head_row // groups == k, fresh[k : k + 1], own_key)
                    own_value = jnp.where(head_row // groups == k, vnew[k : k + 1], own_value)
                own_score = jnp.sum(q.astype(f32) * own_key, axis=1, keepdims=True) * inv_root
                eye = lax.broadcasted_iota(jnp.int32, (heads, heads), 0) == lax.broadcasted_iota(
                    jnp.int32, (heads, heads), 1
                )
                forget = jnp.sum(jnp.where(eye, forget_ref[...], 0.0), axis=1, keepdims=True)
                log_gate = jnp.minimum(forget, 0.0) - jnp.log1p(jnp.exp(-jnp.abs(forget)))
                position = lax.broadcasted_iota(jnp.int32, (heads, span), 1)
                latest = (
                    jnp.sum(jnp.where(position == length - 1, cumlog[...], 0.0), axis=1, keepdims=True)
                    + log_gate
                )
                place = lax.broadcasted_iota(jnp.int32, (heads, chunk), 1)
            if c > 1:
                while len(soft) < c:
                    soft.append(soften(len(soft), raws[len(soft)]))
        for copy in smalls[5:]:
            copy.start()
        out_w_copy.start()
    with jax.named_scope("av"):
        parts = []
        for c in range(chunks):
            if c % (chunks // value_parts) == 0:
                value_copy(c // (chunks // value_parts)).wait()
            if c == 0:
                while len(soft) < chunks:
                    soft.append(soften(len(soft), raws[len(soft)]))
            parts.append(jnp.dot(soft[c][2], both(values, c), preferred_element_type=f32))
        top = own_score
        for chunk_top, _, _ in soft:
            top = jnp.maximum(top, chunk_top)
        own_weight = jnp.exp(own_score - top)
        denominator = own_weight
        weighted = jnp.zeros((heads, key_heads * head_size), f32)
        for (chunk_top, total, _), part in zip(soft, parts):
            scale = jnp.exp(chunk_top - top)
            denominator = denominator + scale * total
            weighted = weighted + scale * part
        mine = weighted[:, :head_size]
        for k in range(1, key_heads):
            mine = jnp.where(
                head_row // groups == k, weighted[:, k * head_size : (k + 1) * head_size], mine
            )
        numerator = mine + own_weight.astype(bf16).astype(f32) * own_value
        att_buf[me] = (numerator / denominator).astype(bf16)

    with jax.named_scope("barsend0"):
        pl.semaphore_wait(barrier, n - 1)
        def send_row(to):
            peer = 2 * to + 1
            remote(0, att_buf.at[me], att_buf.at[me], peer, recv_sem.at[0]).start()

        outward = 1 - 2 * (pair // (pairs // 2))
        for i in range(1, pairs):
            send_row(lax.rem(pair + outward * (pairs - i) + pairs, pairs))
        pl.when(side == 0)(functools.partial(send_row, pair))
        for copy in shared_copies + gate_up_copies + [down_copy, sdown_copy]:
            copy.start()

    def lend(phase, buf, sem):
        return remote(phase, buf.at[0], buf.at[0], me + 1 - 2 * side, sem)

    lent = (lend(1, out_w, recv_sem.at[1]), lend(2, residual_ref, recv_sem.at[2]))
    with jax.named_scope("lend"):
        for copy in smalls[5:]:
            copy.wait()
        out_w_copy.wait()

        @pl.when(side == 0)
        def _():
            for copy in lent:
                copy.start()

    with jax.named_scope("prep"):
        route_scores = route_scores_ref[...]
        gate_weights = (
            route_scores / jnp.sum(route_scores, axis=0, keepdims=True) * routed_scale
        )
        expert_row = lax.broadcasted_iota(jnp.int32, (n, rows), 0)
        share = jnp.zeros((n, rows), f32)
        for k in range(routes_ref.shape[0]):
            share = share + jnp.where(
                routes_ref[k : k + 1] == expert_row, gate_weights[k : k + 1], 0.0
            )
        row_eye = lax.broadcasted_iota(jnp.int32, (rows, rows), 0) == lax.broadcasted_iota(
            jnp.int32, (rows, rows), 1
        )
        shares = [
            jnp.sum(jnp.where(row_eye, share[e : e + 1], 0.0), axis=1, keepdims=True)
            for e in range(n)
        ]

    def project():
        for copy in lent:
            copy.wait_recv()
        with jax.named_scope("arrive0"):
            arrive(0, att_buf, recv_sem.at[0], 0, n - 1)
        with jax.named_scope("oproj_send1"):
            att_wide[...] = att_buf[...].astype(f32).reshape(n * heads, head_size)
            attended = jnp.concatenate(
                [att_wide[pl.ds(h, n, stride=heads), :].astype(bf16) for h in range(heads)], axis=1
            )
            halves = []
            for k in range(2):
                mixed = jnp.dot(attended, out_w[k], preferred_element_type=f32)
                halves.append(widen((residual_ref[k].astype(f32) + mixed).astype(bf16)))
            stream_buf[pair] = widen(join_lanes(halves, width))
            block = stream_buf.at[pair]

            def send_stream(to, core):
                remote(1 + core, block, block, 2 * to + core, stream_sem.at[home]).start()

            send_stream(pair, 0)
            for i in range(pairs - 1):
                to = pick([order[i] for order in targets], pair)
                for core in range(2):
                    send_stream(to, core)

    pl.when(leads)(project)

    @pl.when(side == 0)
    def _():
        sent(0, att_buf, pairs)
        for copy in lent:
            copy.wait_send()

    def stream_sent():
        sent(0, att_buf, pairs - 1)
        sent(1, stream_buf, pairs)
        sent(2, stream_buf, pairs - 1)

    with jax.named_scope("wwait"):
        pltpu.make_async_copy(shared_w, shared_w, key_sem.at[2]).wait()
        pltpu.make_async_copy(gate_up_w, gate_up_w, key_sem.at[3]).wait()

    with jax.named_scope("gateup_send2"):
        weights = (shared_w.at[0], shared_w.at[1], gate_up_w.at[0], gate_up_w.at[1])
        sums = [jnp.zeros((rows, w.shape[0]), f32) for w in weights]
        squares = jnp.zeros((rows, 1), f32)
        firsts = (first_shared.at[0], first_shared.at[1], first_expert.at[0], first_expert.at[1])
        for i in range(turns):
            c = visit(i)
            part = pl.ds(pl.multiple_of(c * wide, wide), wide)
            with jax.named_scope("w%d" % i):
                come = functools.partial(arrive, 1, stream_buf, stream_sem.at[c])
                if i:
                    come(c * pair_per, pair_per)
                else:
                    pl.when(side == 0)(functools.partial(come, 0, pair_per))
                    if pair_per > 1:
                        pl.when(leads)(functools.partial(come, 0, pair_per - 1))
            block = join_lanes(
                [stream_buf[c * pair_per + t] for t in range(pair_per)], 2 * width
            ).astype(f32)
            squares = squares + jnp.sum(block * block, axis=1, keepdims=True)
            scaled = (block * gain_ref[:, part]).astype(bf16)
            sums = [total + dot_t(scaled, w[:, part]) for total, w in zip(sums, weights)]
            if i == turns - 2:
                pl.when(leads)(stream_sent)
            if i == 0:
                for ref, total in zip(firsts, sums):
                    ref[...] = total
                sums = [jnp.zeros_like(total) for total in sums]
        sums = [ref[...] + total for ref, total in zip(firsts, sums)]
        inv_rms = lax.rsqrt(squares * (1.0 / model) + norm_eps)
        sgated, supped, gated, upped = [total * inv_rms for total in sums]

        mid_buf[me] = widen((jax.nn.silu(sgated) * supped).astype(bf16))
        for k in range(per):
            send_mid(k)
        hidden = (jax.nn.silu(gated) * upped).astype(bf16)
    with jax.named_scope("down_send3"):
        down_copy.wait()

        def expert_out(c):
            part = pl.ds(pl.multiple_of(c * wide, wide), wide)
            return jnp.dot(hidden, down_w[:, part], preferred_element_type=f32).astype(bf16)

        def send_block(peer):
            remote(1, eo_src.at[peer], eo_buf.at[me], peer, recv_sem.at[1]).start()

        def put(i, c, out):
            for s in range(per):
                eo_src[c * per + s] = widen(out[:, s * width : (s + 1) * width])
            if i < turns - 1:
                for s in range(per):
                    send_block(c * per + s)
            else:
                for s in range(per - 1):
                    send_block(c * per + s + jnp.where(me - c * per <= s, 1, 0))
            if i:
                for k in range(i * per, min((i + 1) * per, n - 1)):
                    send_mid(k)

        chips = [i + jnp.where(home <= i, 1, 0) for i in range(turns - 1)] + [home]
        put(0, chips[0], expert_out(chips[0]))
        out = expert_out(chips[1])
        for i in range(2, turns):
            following = expert_out(chips[i])
            put(i - 1, chips[i - 1], out)
            out = following
        put(turns - 1, home, out)
        eo_buf[me] = eo_src[me]

    with jax.named_scope("sentwait"):
        sdown_copy.wait()
        sent(0, mid_buf, n - 1)
    with jax.named_scope("arrive2"):
        arrive(0, mid_buf, recv_sem.at[0], 0, n - 1)
    with jax.named_scope("sdown"):
        mid = jnp.concatenate([mid_buf[j] for j in range(n)], axis=1)
        shared_down = sdown_w[...].reshape(mid.shape[1], width)
        mine = stream_buf[pair].astype(f32)
        stream = jnp.where(leads, mine[:, width : 2 * width], mine[:, :width])
        total = stream + jnp.dot(mid, shared_down, preferred_element_type=f32)
    with jax.named_scope("arrive3"):
        sent(1, eo_src, n - 1)
        arrive(1, eo_buf, recv_sem.at[1], 0, n - 1)
    with jax.named_scope("final"):
        for e in range(n):
            total = total + shares[e] * eo_buf[e][:, :width].astype(f32)
        out_ref[...] = total.astype(bf16)


def solution(mesh):
    n = mesh.shape["ep"]

    def on_device(
        queries,
        fresh_token_key,
        value_new,
        forget_logit,
        cache_keys,
        cache_values,
        cache_cumlog,
        lengths,
        residual,
        out_weight,
        norm_gain,
        expert_gate,
        expert_up,
        expert_down,
        shared_gate,
        shared_up,
        shared_down,
        routes,
        route_scores,
    ):
        rows, width = residual.shape
        heads, head_size = queries.shape[1:]
        span = cache_keys.shape[2]
        model = norm_gain.shape[0]
        lanes = -(-width // LANES) * LANES
        mid_lanes = -(-shared_gate.shape[0] // LANES) * LANES
        pair_lanes = -(-2 * width // LANES) * LANES
        turns = model // (2 * max(width, LANES))
        chunks = 4
        hbm = pl.BlockSpec(memory_space=pltpu.HBM)

        def like(a, drop=0):
            return pltpu.VMEM(a.shape[drop:], a.dtype)

        def held(a):
            return pltpu.with_memory_space_constraint(a, pltpu.HBM)

        return pl.pallas_call(
            functools.partial(layer, n),
            out_shape=pltpu.VMEM((rows, width), bf16),
            in_specs=[pl.BlockSpec(memory_space=pl.ANY)] + [hbm] * 18,
            out_specs=pl.BlockSpec(memory_space=pltpu.VMEM),
            scratch_shapes=[
                pltpu.SMEM((1, 1), jnp.int32),
                like(queries),
                like(fresh_token_key),
                like(value_new),
                like(forget_logit),
                pltpu.VMEM((2, *residual.shape), bf16),
                pltpu.VMEM((1, model), f32),
                pltpu.VMEM(routes.shape[::-1], routes.dtype),
                pltpu.VMEM(route_scores.shape[::-1], f32),
                like(cache_keys, 1),
                like(cache_values, 1),
                like(cache_cumlog, 1),
                pltpu.VMEM((2, *out_weight.shape), bf16),
                pltpu.VMEM((2, *expert_gate.shape[1:]), bf16),
                like(expert_down, 1),
                pltpu.VMEM((2, *shared_gate.shape), bf16),
                pltpu.VMEM((n, mid_lanes, width), bf16),
                pltpu.VMEM((n, heads, head_size), bf16),
                pltpu.VMEM((n * heads, head_size), f32),
                pltpu.VMEM((n // 2, rows, pair_lanes), bf16),
                pltpu.VMEM((n, rows, mid_lanes), bf16),
                pltpu.VMEM((n, rows, lanes), bf16),
                pltpu.VMEM((n, rows, lanes), bf16),
                pltpu.VMEM((2, rows, shared_gate.shape[0]), f32),
                pltpu.VMEM((2, rows, expert_gate.shape[1]), f32),
                pltpu.SemaphoreType.DMA((5,)),
                pltpu.SemaphoreType.DMA((chunks,)),
                pltpu.SemaphoreType.DMA((2 + 1,)),
                pltpu.SemaphoreType.DMA((3,)),
                pltpu.SemaphoreType.DMA((3,)),
                pltpu.SemaphoreType.DMA((turns,)),
            ],
            compiler_params=pltpu.CompilerParams(
                collective_id=0, has_side_effects=True, vmem_limit_bytes=VMEM_LIMIT
            ),
            name="layer",
        )(
            lengths.reshape(1, 1),
            *map(
                held,
                (
                    queries,
                    fresh_token_key,
                    value_new,
                    forget_logit,
                    residual,
                    norm_gain.reshape(1, -1),
                    routes.T,
                    route_scores.T,
                    cache_keys,
                    cache_values,
                    cache_cumlog,
                    out_weight,
                    expert_gate,
                    expert_up,
                    expert_down,
                    shared_gate,
                    shared_up,
                    shared_down.reshape(n, -1, width),
                ),
            ),
        )

    placed = (
        P(("grp", "ep"), None, None),
        P(("grp", "ep"), None, None),
        P(("grp", "ep"), None, None),
        P(("grp", "ep"), None),
        P(("grp", "ep"), None, None, None),
        P(("grp", "ep"), None, None, None),
        P(("grp", "ep"), None, None),
        P(("grp", "ep")),
        P("grp", "ep"),
        P(None, "ep"),
        P(),
        P("ep", None, None),
        P("ep", None, None),
        P("ep", None, None),
        P("ep", None),
        P("ep", None),
        P(None, "ep"),
        P("grp", None),
        P("grp", None),
    )
    return jax.shard_map(
        on_device, mesh=mesh, in_specs=placed, out_specs=P("grp", "ep"), check_vma=False
    )
```

```python
import functools

import jax
import jax.numpy as jnp
from jax import lax
from jax.experimental import pallas as pl
from jax.experimental.pallas import tpu as pltpu
from jax.sharding import PartitionSpec as P

norm_eps = 1e-06
routed_scale = 2.5
contract_last = (((1,), (1,)), ((), ()))
LANES = 128
VMEM_LIMIT = 48 * 1024 * 1024
f32 = jnp.float32
bf16 = jnp.bfloat16


def dot_t(a, b):
    return lax.dot_general(a, b, contract_last, preferred_element_type=f32)


def join_lanes(blocks, width):
    if width % LANES == 0:
        return jnp.concatenate([b.astype(bf16) for b in blocks], axis=1)
    rows = blocks[0].shape[0]
    total = len(blocks) * width
    lane = lax.broadcasted_iota(jnp.int32, (rows, LANES), 1)
    pieces = [jnp.zeros((rows, LANES), f32) for _ in range(-(-total // LANES))]
    for k, block in enumerate(blocks):
        at, shift = divmod(k * width, LANES)
        moved = jnp.where(lane < width, block.astype(f32), 0.0)
        if shift:
            moved = pltpu.roll(moved, shift, 1)
        if shift + width <= LANES:
            pieces[at] = pieces[at] + moved
        else:
            pieces[at] = pieces[at] + jnp.where(lane >= shift, moved, 0.0)
            pieces[at + 1] = pieces[at + 1] + jnp.where(lane < shift, moved, 0.0)
    return jnp.concatenate([p.astype(bf16) for p in pieces], axis=1)[:, :total]


def widen(block):
    rows, width = block.shape
    short = -width % LANES
    if not short:
        return block
    return jnp.concatenate([block, jnp.zeros((rows, short), block.dtype)], axis=1)


def hops(a, b, sides):
    return abs(a // sides - b // sides) + (a % sides != b % sides)


def visit_order(home, turns):
    sides = 2 - turns % 2

    def late(c):
        sent = max(hops(c, turns - 1, sides), hops(c, 0, sides) - 1)
        return (c != home, 0.55 * abs(c // sides - home // sides) + 0.6 * (c % sides != home % sides) - 0.2 * (c // sides))

    return sorted(range(turns), key=late)


def send_order(home, pairs):
    sides = 2 - pairs % 2
    return sorted((c for c in range(pairs) if c != home), key=lambda c: -c)


def pick(table, at):
    entry = jnp.int32(table[0])
    for h in range(1, len(table)):
        entry = jnp.where(at == h, table[h], entry)
    return entry


def layer(
    n,
    lengths_hbm,
    q_hbm,
    fresh_hbm,
    vnew_hbm,
    forget_hbm,
    residual_hbm,
    gain_hbm,
    routes_hbm,
    route_scores_hbm,
    keys_hbm,
    values_hbm,
    cumlog_hbm,
    out_w_hbm,
    gate_hbm,
    up_hbm,
    down_hbm,
    sgate_hbm,
    sup_hbm,
    sdown_hbm,
    out_ref,
    lengths_ref,
    q_ref,
    fresh_ref,
    vnew_ref,
    forget_ref,
    residual_ref,
    gain_ref,
    routes_ref,
    route_scores_ref,
    keys,
    values,
    cumlog,
    out_w,
    gate_up_w,
    down_w,
    shared_w,
    sdown_w,
    att_buf,
    att_wide,
    stream_buf,
    mid_buf,
    eo_src,
    eo_buf,
    first_shared,
    first_expert,
    small_sem,
    key_sem,
    value_sem,
    send_sem,
    recv_sem,
    stream_sem,
):
    me = lax.axis_index("ep")
    heads, head_size = q_ref.shape[1:]
    key_heads, span = keys.shape[:2]
    groups = heads // key_heads
    rows, width = residual_ref.shape[1:]
    ff, model = gate_up_w.shape[1:]
    shared_width = shared_w.shape[1]
    chunks = key_sem.shape[0]
    chunk = span // chunks

    def key_copy(c):
        part = pl.ds(c * chunk, chunk)
        return pltpu.make_async_copy(keys_hbm.at[0, :, part], keys.at[:, part], key_sem.at[c])

    value_parts = value_sem.shape[0] - 1
    late_values = 1
    value_chunk = span // value_parts

    def value_copy(c):
        part = pl.ds(c * value_chunk, value_chunk)
        return pltpu.make_async_copy(values_hbm.at[0, :, part], values.at[:, part], value_sem.at[c])

    cumlog_copy = pltpu.make_async_copy(cumlog_hbm.at[0], cumlog, value_sem.at[2])
    out_w_copy = pltpu.make_async_copy(
        out_w_hbm, out_w.at[lax.rem(me, 2)], key_sem.at[1]
    )
    down_copy = pltpu.make_async_copy(down_hbm.at[0], down_w, key_sem.at[0])
    sdown_copy = pltpu.make_async_copy(
        sdown_hbm, sdown_w.at[:, pl.ds(0, sdown_hbm.shape[1])], small_sem.at[4]
    )

    def pair_copies(first, second, both, sem):
        return [
            pltpu.make_async_copy(src, both.at[k], sem) for k, src in enumerate((first, second))
        ]

    shared_copies = pair_copies(sgate_hbm, sup_hbm, shared_w, key_sem.at[2])
    gate_up_copies = pair_copies(gate_hbm.at[0], up_hbm.at[0], gate_up_w, key_sem.at[3])

    smalls = [
        pltpu.make_async_copy(src, dst, small_sem.at[i % 5])
        for i, (src, dst) in enumerate(
            (
                (q_hbm, q_ref),
                (fresh_hbm, fresh_ref),
                (vnew_hbm, vnew_ref),
                (forget_hbm, forget_ref),
                (lengths_hbm, lengths_ref),
                (routes_hbm, routes_ref),
                (route_scores_hbm, route_scores_ref),
                (residual_hbm, residual_ref.at[lax.rem(me, 2)]),
                (gain_hbm, gain_ref),
            )
        )
    ]
    key_copy(0).start()
    for copy in smalls[:5]:
        copy.start()
    cumlog_copy.start()
    for c in range(1, chunks):
        key_copy(c).start()
    for c in range(value_parts - late_values):
        value_copy(c).start()
    sdown_w[...] = jnp.zeros_like(sdown_w)
    barrier = pltpu.get_barrier_semaphore()

    with jax.named_scope("greet"):
        for i in range(1, n):
            pl.semaphore_signal(barrier, inc=1, device_id={"ep": lax.rem(me + i, n)})

    wide = 2 * max(width, LANES)
    per = wide // width
    pairs, pair_per = n // 2, per // 2
    pair, side = me // 2, lax.rem(me, 2)
    leads = side == 1
    turns = model // wide
    home = me // per
    toward = 1 - 2 * (home // (turns // 2))

    def remote(phase, src, dst, peer, sem):
        return pltpu.make_async_remote_copy(
            src_ref=src,
            dst_ref=dst,
            send_sem=send_sem.at[phase],
            recv_sem=sem,
            device_id={"ep": peer},
        )

    def arrive(phase, buf, sem, first, count):
        blocks = buf.at[pl.ds(first, count)]
        remote(phase, blocks, blocks, me, sem).wait_recv()

    def sent(phase, buf, count):
        blocks = buf.at[pl.ds(0, count)]
        remote(phase, blocks, blocks, me, recv_sem.at[0]).wait_send()

    visits = [visit_order(h, turns) for h in range(turns)]
    targets = [send_order(h, pairs) for h in range(pairs)]

    def visit(i):
        return pick([order[i] for order in visits], home)

    def send_mid(k):
        peer = k + jnp.where(me <= k, 1, 0)
        remote(0, mid_buf.at[me], mid_buf.at[me], peer, recv_sem.at[0]).start()

    inv_root = head_size ** (-0.5)
    head_row = lax.broadcasted_iota(jnp.int32, (heads, head_size), 0)
    with jax.named_scope("smallwait"):
        smalls[0].wait()
    q = q_ref[0]
    q_wide = jnp.concatenate(
        [jnp.where(head_row // groups == k, q, jnp.zeros_like(q)) for k in range(key_heads)],
        axis=1,
    )

    def both(ref, c):
        part = slice(c * chunk, (c + 1) * chunk)
        return jnp.concatenate([ref[k, part] for k in range(key_heads)], axis=1)

    def raw_score(c):
        key_copy(c).wait()
        if c < late_values:
            value_copy(value_parts - late_values + c).start()
        return dot_t(q_wide, both(keys, c))

    def soften(c, raw):
        score = raw * inv_root + latest - cumlog[:, c * chunk : (c + 1) * chunk]
        score = jnp.where(place + c * chunk < length, score, -jnp.inf)
        top = jnp.maximum(own_score, jnp.max(score, axis=1, keepdims=True))
        weight = jnp.exp(score - top)
        return top, jnp.sum(weight, axis=1, keepdims=True), weight.astype(bf16)

    raws, soft = [], []
    with jax.named_scope("score"):
        for c in range(chunks):
            raws.append(raw_score(c))
            if c == 1:
                for copy in smalls[1:5]:
                    copy.wait()
                cumlog_copy.wait()
                length = lengths_ref[0, 0]
                fresh, vnew = fresh_ref[0].astype(f32), vnew_ref[0].astype(f32)
                own_key, own_value = fresh[0:1], vnew[0:1]
                for k in range(1, key_heads):
                    own_key = jnp.where(head_row // groups == k, fresh[k : k + 1], own_key)
                    own_value = jnp.where(head_row // groups == k, vnew[k : k + 1], own_value)
                own_score = jnp.sum(q.astype(f32) * own_key, axis=1, keepdims=True) * inv_root
                eye = lax.broadcasted_iota(jnp.int32, (heads, heads), 0) == lax.broadcasted_iota(
                    jnp.int32, (heads, heads), 1
                )
                forget = jnp.sum(jnp.where(eye, forget_ref[...], 0.0), axis=1, keepdims=True)
                log_gate = jnp.minimum(forget, 0.0) - jnp.log1p(jnp.exp(-jnp.abs(forget)))
                position = lax.broadcasted_iota(jnp.int32, (heads, span), 1)
                latest = (
                    jnp.sum(jnp.where(position == length - 1, cumlog[...], 0.0), axis=1, keepdims=True)
                    + log_gate
                )
                place = lax.broadcasted_iota(jnp.int32, (heads, chunk), 1)
            if c > 1:
                while len(soft) < c:
                    soft.append(soften(len(soft), raws[len(soft)]))
        for copy in smalls[5:]:
            copy.start()
        out_w_copy.start()
    with jax.named_scope("av"):
        parts = []
        for c in range(chunks):
            if c % (chunks // value_parts) == 0:
                value_copy(c // (chunks // value_parts)).wait()
            if c == 0:
                while len(soft) < chunks:
                    soft.append(soften(len(soft), raws[len(soft)]))
            parts.append(jnp.dot(soft[c][2], both(values, c), preferred_element_type=f32))
        top = own_score
        for chunk_top, _, _ in soft:
            top = jnp.maximum(top, chunk_top)
        own_weight = jnp.exp(own_score - top)
        denominator = own_weight
        weighted = jnp.zeros((heads, key_heads * head_size), f32)
        for (chunk_top, total, _), part in zip(soft, parts):
            scale = jnp.exp(chunk_top - top)
            denominator = denominator + scale * total
            weighted = weighted + scale * part
        mine = weighted[:, :head_size]
        for k in range(1, key_heads):
            mine = jnp.where(
                head_row // groups == k, weighted[:, k * head_size : (k + 1) * head_size], mine
            )
        numerator = mine + own_weight.astype(bf16).astype(f32) * own_value
        att_buf[me] = (numerator / denominator).astype(bf16)

    with jax.named_scope("barsend0"):
        pl.semaphore_wait(barrier, n - 1)
        def send_row(to):
            peer = 2 * to + 1
            remote(0, att_buf.at[me], att_buf.at[me], peer, recv_sem.at[0]).start()

        outward = 1 - 2 * (pair // (pairs // 2))
        for i in range(1, pairs):
            send_row(lax.rem(pair + outward * (pairs - i) + pairs, pairs))
        pl.when(side == 0)(functools.partial(send_row, pair))
        for copy in shared_copies + gate_up_copies + [down_copy, sdown_copy]:
            copy.start()

    def lend(phase, buf, sem):
        return remote(phase, buf.at[0], buf.at[0], me + 1 - 2 * side, sem)

    lent = (lend(1, out_w, recv_sem.at[1]), lend(2, residual_ref, recv_sem.at[2]))
    with jax.named_scope("lend"):
        for copy in smalls[5:]:
            copy.wait()
        out_w_copy.wait()

        @pl.when(side == 0)
        def _():
            for copy in lent:
                copy.start()

    with jax.named_scope("prep"):
        route_scores = route_scores_ref[...]
        gate_weights = (
            route_scores / jnp.sum(route_scores, axis=0, keepdims=True) * routed_scale
        )
        expert_row = lax.broadcasted_iota(jnp.int32, (n, rows), 0)
        share = jnp.zeros((n, rows), f32)
        for k in range(routes_ref.shape[0]):
            share = share + jnp.where(
                routes_ref[k : k + 1] == expert_row, gate_weights[k : k + 1], 0.0
            )
        row_eye = lax.broadcasted_iota(jnp.int32, (rows, rows), 0) == lax.broadcasted_iota(
            jnp.int32, (rows, rows), 1
        )
        shares = [
            jnp.sum(jnp.where(row_eye, share[e : e + 1], 0.0), axis=1, keepdims=True)
            for e in range(n)
        ]

    def project():
        for copy in lent:
            copy.wait_recv()
        with jax.named_scope("arrive0"):
            arrive(0, att_buf, recv_sem.at[0], 0, n - 1)
        with jax.named_scope("oproj_send1"):
            att_wide[...] = att_buf[...].astype(f32).reshape(n * heads, head_size)
            attended = jnp.concatenate(
                [att_wide[pl.ds(h, n, stride=heads), :].astype(bf16) for h in range(heads)], axis=1
            )
            halves = []
            for k in range(2):
                mixed = jnp.dot(attended, out_w[k], preferred_element_type=f32)
                halves.append(widen((residual_ref[k].astype(f32) + mixed).astype(bf16)))
            stream_buf[pair] = widen(join_lanes(halves, width))
            block = stream_buf.at[pair]

            def send_stream(to, core):
                remote(1 + core, block, block, 2 * to + core, stream_sem.at[home]).start()

            send_stream(pair, 0)
            for i in range(pairs - 1):
                to = pick([order[i] for order in targets], pair)
                for core in range(2):
                    send_stream(to, core)

    pl.when(leads)(project)

    @pl.when(side == 0)
    def _():
        sent(0, att_buf, pairs)
        for copy in lent:
            copy.wait_send()

    def stream_sent():
        sent(0, att_buf, pairs - 1)
        sent(1, stream_buf, pairs)
        sent(2, stream_buf, pairs - 1)

    with jax.named_scope("wwait"):
        pltpu.make_async_copy(shared_w, shared_w, key_sem.at[2]).wait()
        pltpu.make_async_copy(gate_up_w, gate_up_w, key_sem.at[3]).wait()

    with jax.named_scope("gateup_send2"):
        weights = (shared_w.at[0], shared_w.at[1], gate_up_w.at[0], gate_up_w.at[1])
        sums = [jnp.zeros((rows, w.shape[0]), f32) for w in weights]
        squares = jnp.zeros((rows, 1), f32)
        firsts = (first_shared.at[0], first_shared.at[1], first_expert.at[0], first_expert.at[1])
        for i in range(turns):
            c = visit(i)
            part = pl.ds(pl.multiple_of(c * wide, wide), wide)
            with jax.named_scope("w%d" % i):
                if i == turns - 2:
                    down_copy.wait()
                    sdown_copy.wait()
                come = functools.partial(arrive, 1, stream_buf, stream_sem.at[c])
                if i:
                    come(c * pair_per, pair_per)
                else:
                    pl.when(side == 0)(functools.partial(come, 0, pair_per))
                    if pair_per > 1:
                        pl.when(leads)(functools.partial(come, 0, pair_per - 1))
            block = join_lanes(
                [stream_buf[c * pair_per + t] for t in range(pair_per)], 2 * width
            ).astype(f32)
            squares = squares + jnp.sum(block * block, axis=1, keepdims=True)
            scaled = (block * gain_ref[:, part]).astype(bf16)
            sums = [total + dot_t(scaled, w[:, part]) for total, w in zip(sums, weights)]
            if i == turns - 2:
                pl.when(leads)(stream_sent)
            if i == 0:
                for ref, total in zip(firsts, sums):
                    ref[...] = total
                sums = [jnp.zeros_like(total) for total in sums]
        sums = [ref[...] + total for ref, total in zip(firsts, sums)]
        inv_rms = lax.rsqrt(squares * (1.0 / model) + norm_eps)
        sgated, supped, gated, upped = [total * inv_rms for total in sums]

        mid_buf[me] = widen((jax.nn.silu(sgated) * supped).astype(bf16))
        for k in range(per):
            send_mid(k)
        hidden = (jax.nn.silu(gated) * upped).astype(bf16)
    with jax.named_scope("down_send3"):

        def expert_out(c):
            part = pl.ds(pl.multiple_of(c * wide, wide), wide)
            return jnp.dot(hidden, down_w[:, part], preferred_element_type=f32).astype(bf16)

        def send_block(peer):
            remote(1, eo_src.at[peer], eo_buf.at[me], peer, recv_sem.at[1]).start()

        def put(i, c, out):
            for s in range(per):
                eo_src[c * per + s] = widen(out[:, s * width : (s + 1) * width])
            if i < turns - 1:
                for s in range(per):
                    send_block(c * per + s)
            else:
                for s in range(per - 1):
                    send_block(c * per + s + jnp.where(me - c * per <= s, 1, 0))
            if i:
                for k in range(i * per, min((i + 1) * per, n - 1)):
                    send_mid(k)

        chips = [i + jnp.where(home <= i, 1, 0) for i in range(turns - 1)] + [home]
        put(0, chips[0], expert_out(chips[0]))
        out = expert_out(chips[1])
        for i in range(2, turns):
            following = expert_out(chips[i])
            put(i - 1, chips[i - 1], out)
            out = following
        put(turns - 1, home, out)
        eo_buf[me] = eo_src[me]

    with jax.named_scope("sentwait"):
        sent(0, mid_buf, n - 1)
    with jax.named_scope("arrive2"):
        arrive(0, mid_buf, recv_sem.at[0], 0, n - 1)
    with jax.named_scope("sdown"):
        mid = jnp.concatenate([mid_buf[j] for j in range(n)], axis=1)
        shared_down = sdown_w[...].reshape(mid.shape[1], width)
        mine = stream_buf[pair].astype(f32)
        stream = jnp.where(leads, mine[:, width : 2 * width], mine[:, :width])
        total = stream + jnp.dot(mid, shared_down, preferred_element_type=f32)
    with jax.named_scope("arrive3"):
        sent(1, eo_src, n - 1)
        arrive(1, eo_buf, recv_sem.at[1], 0, n - 1)
    with jax.named_scope("final"):
        for e in range(n):
            total = total + shares[e] * eo_buf[e][:, :width].astype(f32)
        out_ref[...] = total.astype(bf16)


def solution(mesh):
    n = mesh.shape["ep"]

    def on_device(
        queries,
        fresh_token_key,
        value_new,
        forget_logit,
        cache_keys,
        cache_values,
        cache_cumlog,
        lengths,
        residual,
        out_weight,
        norm_gain,
        expert_gate,
        expert_up,
        expert_down,
        shared_gate,
        shared_up,
        shared_down,
        routes,
        route_scores,
    ):
        rows, width = residual.shape
        heads, head_size = queries.shape[1:]
        span = cache_keys.shape[2]
        model = norm_gain.shape[0]
        lanes = -(-width // LANES) * LANES
        mid_lanes = -(-shared_gate.shape[0] // LANES) * LANES
        pair_lanes = -(-2 * width // LANES) * LANES
        turns = model // (2 * max(width, LANES))
        chunks = 4
        hbm = pl.BlockSpec(memory_space=pltpu.HBM)

        def like(a, drop=0):
            return pltpu.VMEM(a.shape[drop:], a.dtype)

        def held(a):
            return pltpu.with_memory_space_constraint(a, pltpu.HBM)

        return pl.pallas_call(
            functools.partial(layer, n),
            out_shape=pltpu.VMEM((rows, width), bf16),
            in_specs=[pl.BlockSpec(memory_space=pl.ANY)] + [hbm] * 18,
            out_specs=pl.BlockSpec(memory_space=pltpu.VMEM),
            scratch_shapes=[
                pltpu.SMEM((1, 1), jnp.int32),
                like(queries),
                like(fresh_token_key),
                like(value_new),
                like(forget_logit),
                pltpu.VMEM((2, *residual.shape), bf16),
                pltpu.VMEM((1, model), f32),
                pltpu.VMEM(routes.shape[::-1], routes.dtype),
                pltpu.VMEM(route_scores.shape[::-1], f32),
                like(cache_keys, 1),
                like(cache_values, 1),
                like(cache_cumlog, 1),
                pltpu.VMEM((2, *out_weight.shape), bf16),
                pltpu.VMEM((2, *expert_gate.shape[1:]), bf16),
                like(expert_down, 1),
                pltpu.VMEM((2, *shared_gate.shape), bf16),
                pltpu.VMEM((n, mid_lanes, width), bf16),
                pltpu.VMEM((n, heads, head_size), bf16),
                pltpu.VMEM((n * heads, head_size), f32),
                pltpu.VMEM((n // 2, rows, pair_lanes), bf16),
                pltpu.VMEM((n, rows, mid_lanes), bf16),
                pltpu.VMEM((n, rows, lanes), bf16),
                pltpu.VMEM((n, rows, lanes), bf16),
                pltpu.VMEM((2, rows, shared_gate.shape[0]), f32),
                pltpu.VMEM((2, rows, expert_gate.shape[1]), f32),
                pltpu.SemaphoreType.DMA((5,)),
                pltpu.SemaphoreType.DMA((chunks,)),
                pltpu.SemaphoreType.DMA((2 + 1,)),
                pltpu.SemaphoreType.DMA((3,)),
                pltpu.SemaphoreType.DMA((3,)),
                pltpu.SemaphoreType.DMA((turns,)),
            ],
            compiler_params=pltpu.CompilerParams(
                collective_id=0, has_side_effects=True, vmem_limit_bytes=VMEM_LIMIT
            ),
            name="layer",
        )(
            lengths.reshape(1, 1),
            *map(
                held,
                (
                    queries,
                    fresh_token_key,
                    value_new,
                    forget_logit,
                    residual,
                    norm_gain.reshape(1, -1),
                    routes.T,
                    route_scores.T,
                    cache_keys,
                    cache_values,
                    cache_cumlog,
                    out_weight,
                    expert_gate,
                    expert_up,
                    expert_down,
                    shared_gate,
                    shared_up,
                    shared_down.reshape(n, -1, width),
                ),
            ),
        )

    placed = (
        P(("grp", "ep"), None, None),
        P(("grp", "ep"), None, None),
        P(("grp", "ep"), None, None),
        P(("grp", "ep"), None),
        P(("grp", "ep"), None, None, None),
        P(("grp", "ep"), None, None, None),
        P(("grp", "ep"), None, None),
        P(("grp", "ep")),
        P("grp", "ep"),
        P(None, "ep"),
        P(),
        P("ep", None, None),
        P("ep", None, None),
        P("ep", None, None),
        P("ep", None),
        P("ep", None),
        P(None, "ep"),
        P("grp", None),
        P("grp", None),
    )
    return jax.shard_map(
        on_device, mesh=mesh, in_specs=placed, out_specs=P("grp", "ep"), check_vma=False
    )
```

```python
import functools

import jax
import jax.numpy as jnp
from jax import lax
from jax.experimental import pallas as pl
from jax.experimental.pallas import tpu as pltpu
from jax.sharding import PartitionSpec as P

norm_eps = 1e-06
routed_scale = 2.5
contract_last = (((1,), (1,)), ((), ()))
LANES = 128
VMEM_LIMIT = 48 * 1024 * 1024
f32 = jnp.float32
bf16 = jnp.bfloat16


def dot_t(a, b):
    return lax.dot_general(a, b, contract_last, preferred_element_type=f32)


def join_lanes(blocks, width):
    if width % LANES == 0:
        return jnp.concatenate([b.astype(bf16) for b in blocks], axis=1)
    rows = blocks[0].shape[0]
    total = len(blocks) * width
    lane = lax.broadcasted_iota(jnp.int32, (rows, LANES), 1)
    pieces = [jnp.zeros((rows, LANES), f32) for _ in range(-(-total // LANES))]
    for k, block in enumerate(blocks):
        at, shift = divmod(k * width, LANES)
        moved = jnp.where(lane < width, block.astype(f32), 0.0)
        if shift:
            moved = pltpu.roll(moved, shift, 1)
        if shift + width <= LANES:
            pieces[at] = pieces[at] + moved
        else:
            pieces[at] = pieces[at] + jnp.where(lane >= shift, moved, 0.0)
            pieces[at + 1] = pieces[at + 1] + jnp.where(lane < shift, moved, 0.0)
    return jnp.concatenate([p.astype(bf16) for p in pieces], axis=1)[:, :total]


def widen(block):
    rows, width = block.shape
    short = -width % LANES
    if not short:
        return block
    return jnp.concatenate([block, jnp.zeros((rows, short), block.dtype)], axis=1)


def hops(a, b, sides):
    return abs(a // sides - b // sides) + (a % sides != b % sides)


def visit_order(home, turns):
    sides = 2 - turns % 2

    def late(c):
        sent = max(hops(c, turns - 1, sides), hops(c, 0, sides) - 1)
        return (c != home, 0.55 * abs(c // sides - home // sides) + 0.6 * (c % sides != home % sides) - 0.2 * (c // sides))

    return sorted(range(turns), key=late)


def pick(table, at):
    entry = jnp.int32(table[0])
    for h in range(1, len(table)):
        entry = jnp.where(at == h, table[h], entry)
    return entry


def layer(
    n,
    lengths_hbm,
    q_hbm,
    fresh_hbm,
    vnew_hbm,
    forget_hbm,
    residual_hbm,
    gain_hbm,
    routes_hbm,
    route_scores_hbm,
    keys_hbm,
    values_hbm,
    cumlog_hbm,
    out_w_hbm,
    gate_hbm,
    up_hbm,
    down_hbm,
    sgate_hbm,
    sup_hbm,
    sdown_hbm,
    out_ref,
    lengths_ref,
    q_ref,
    fresh_ref,
    vnew_ref,
    forget_ref,
    residual_ref,
    gain_ref,
    routes_ref,
    route_scores_ref,
    keys,
    values,
    cumlog,
    out_w,
    gate_up_w,
    down_w,
    shared_w,
    sdown_w,
    att_buf,
    att_wide,
    stream_buf,
    mid_buf,
    eo_src,
    eo_buf,
    first_shared,
    first_expert,
    small_sem,
    key_sem,
    value_sem,
    send_sem,
    recv_sem,
    stream_sem,
):
    me = lax.axis_index("ep")
    heads, head_size = q_ref.shape[1:]
    key_heads, span = keys.shape[:2]
    groups = heads // key_heads
    rows, width = residual_ref.shape[1:]
    ff, model = gate_up_w.shape[1:]
    shared_width = shared_w.shape[1]
    chunks = key_sem.shape[0]
    chunk = span // chunks

    def key_copy(c):
        part = pl.ds(c * chunk, chunk)
        return pltpu.make_async_copy(keys_hbm.at[0, :, part], keys.at[:, part], key_sem.at[c])

    value_parts = value_sem.shape[0] - 1
    late_values = 1
    value_chunk = span // value_parts

    def value_copy(c):
        part = pl.ds(c * value_chunk, value_chunk)
        return pltpu.make_async_copy(values_hbm.at[0, :, part], values.at[:, part], value_sem.at[c])

    cumlog_copy = pltpu.make_async_copy(cumlog_hbm.at[0], cumlog, value_sem.at[2])
    out_w_copy = pltpu.make_async_copy(
        out_w_hbm, out_w.at[lax.rem(me, 2)], key_sem.at[1]
    )
    down_copy = pltpu.make_async_copy(down_hbm.at[0], down_w, key_sem.at[0])
    sdown_copy = pltpu.make_async_copy(
        sdown_hbm, sdown_w.at[:, pl.ds(0, sdown_hbm.shape[1])], small_sem.at[4]
    )

    def pair_copies(first, second, both, sem):
        return [
            pltpu.make_async_copy(src, both.at[k], sem) for k, src in enumerate((first, second))
        ]

    shared_copies = pair_copies(sgate_hbm, sup_hbm, shared_w, key_sem.at[2])
    gate_up_copies = pair_copies(gate_hbm.at[0], up_hbm.at[0], gate_up_w, key_sem.at[3])

    smalls = [
        pltpu.make_async_copy(src, dst, small_sem.at[i % 5])
        for i, (src, dst) in enumerate(
            (
                (q_hbm, q_ref),
                (fresh_hbm, fresh_ref),
                (vnew_hbm, vnew_ref),
                (forget_hbm, forget_ref),
                (lengths_hbm, lengths_ref),
                (routes_hbm, routes_ref),
                (route_scores_hbm, route_scores_ref),
                (residual_hbm, residual_ref.at[lax.rem(me, 2)]),
                (gain_hbm, gain_ref),
            )
        )
    ]
    key_copy(0).start()
    smalls[0].start()
    sdown_w[...] = jnp.zeros_like(sdown_w)
    barrier = pltpu.get_barrier_semaphore()

    with jax.named_scope("greet"):
        for i in range(1, n):
            pl.semaphore_signal(barrier, inc=1, device_id={"ep": lax.rem(me + i, n)})
    for copy in smalls[1:5]:
        copy.start()
    cumlog_copy.start()
    for c in range(1, chunks):
        key_copy(c).start()
    for c in range(value_parts - late_values):
        value_copy(c).start()

    wide = 2 * max(width, LANES)
    per = wide // width
    pairs, pair_per = n // 2, per // 2
    pair, side = me // 2, lax.rem(me, 2)
    leads = side == 1
    turns = model // wide
    home = me // per
    toward = 1 - 2 * (home // (turns // 2))

    def remote(phase, src, dst, peer, sem):
        return pltpu.make_async_remote_copy(
            src_ref=src,
            dst_ref=dst,
            send_sem=send_sem.at[phase],
            recv_sem=sem,
            device_id={"ep": peer},
        )

    def arrive(phase, buf, sem, first, count):
        blocks = buf.at[pl.ds(first, count)]
        remote(phase, blocks, blocks, me, sem).wait_recv()

    def sent(phase, buf, count):
        blocks = buf.at[pl.ds(0, count)]
        remote(phase, blocks, blocks, me, recv_sem.at[0]).wait_send()

    visits = [visit_order(h, turns) for h in range(turns)]

    def visit(i):
        return pick([order[i] for order in visits], home)

    def send_mid(k):
        peer = k + jnp.where(me <= k, 1, 0)
        remote(0, mid_buf.at[me], mid_buf.at[me], peer, recv_sem.at[0]).start()

    inv_root = head_size ** (-0.5)
    head_row = lax.broadcasted_iota(jnp.int32, (heads, head_size), 0)
    with jax.named_scope("smallwait"):
        smalls[0].wait()
    q = q_ref[0]
    q_wide = jnp.concatenate(
        [jnp.where(head_row // groups == k, q, jnp.zeros_like(q)) for k in range(key_heads)],
        axis=1,
    )

    def both(ref, c):
        part = slice(c * chunk, (c + 1) * chunk)
        return jnp.concatenate([ref[k, part] for k in range(key_heads)], axis=1)

    def raw_score(c):
        key_copy(c).wait()
        if c < late_values:
            value_copy(value_parts - late_values + c).start()
        return dot_t(q_wide, both(keys, c))

    def soften(c, raw):
        score = raw * inv_root + latest - cumlog[:, c * chunk : (c + 1) * chunk]
        score = jnp.where(place + c * chunk < length, score, -jnp.inf)
        top = jnp.maximum(own_score, jnp.max(score, axis=1, keepdims=True))
        weight = jnp.exp(score - top)
        return top, jnp.sum(weight, axis=1, keepdims=True), weight.astype(bf16)

    raws, soft = [], []
    with jax.named_scope("score"):
        for c in range(chunks):
            raws.append(raw_score(c))
            if c == 1:
                for copy in smalls[1:5]:
                    copy.wait()
                cumlog_copy.wait()
                length = lengths_ref[0, 0]
                fresh, vnew = fresh_ref[0].astype(f32), vnew_ref[0].astype(f32)
                own_key, own_value = fresh[0:1], vnew[0:1]
                for k in range(1, key_heads):
                    own_key = jnp.where(head_row // groups == k, fresh[k : k + 1], own_key)
                    own_value = jnp.where(head_row // groups == k, vnew[k : k + 1], own_value)
                own_score = jnp.sum(q.astype(f32) * own_key, axis=1, keepdims=True) * inv_root
                eye = lax.broadcasted_iota(jnp.int32, (heads, heads), 0) == lax.broadcasted_iota(
                    jnp.int32, (heads, heads), 1
                )
                forget = jnp.sum(jnp.where(eye, forget_ref[...], 0.0), axis=1, keepdims=True)
                log_gate = jnp.minimum(forget, 0.0) - jnp.log1p(jnp.exp(-jnp.abs(forget)))
                position = lax.broadcasted_iota(jnp.int32, (heads, span), 1)
                latest = (
                    jnp.sum(jnp.where(position == length - 1, cumlog[...], 0.0), axis=1, keepdims=True)
                    + log_gate
                )
                place = lax.broadcasted_iota(jnp.int32, (heads, chunk), 1)
            if c > 1:
                while len(soft) < c:
                    soft.append(soften(len(soft), raws[len(soft)]))
        for copy in smalls[5:]:
            copy.start()
        out_w_copy.start()
    with jax.named_scope("av"):
        parts = []
        for c in range(chunks):
            if c % (chunks // value_parts) == 0:
                value_copy(c // (chunks // value_parts)).wait()
            if c == 0:
                while len(soft) < chunks:
                    soft.append(soften(len(soft), raws[len(soft)]))
            parts.append(jnp.dot(soft[c][2], both(values, c), preferred_element_type=f32))
        top = own_score
        for chunk_top, _, _ in soft:
            top = jnp.maximum(top, chunk_top)
        own_weight = jnp.exp(own_score - top)
        denominator = own_weight
        weighted = jnp.zeros((heads, key_heads * head_size), f32)
        for (chunk_top, total, _), part in zip(soft, parts):
            scale = jnp.exp(chunk_top - top)
            denominator = denominator + scale * total
            weighted = weighted + scale * part
        mine = weighted[:, :head_size]
        for k in range(1, key_heads):
            mine = jnp.where(
                head_row // groups == k, weighted[:, k * head_size : (k + 1) * head_size], mine
            )
        numerator = mine + own_weight.astype(bf16).astype(f32) * own_value
        att_buf[me] = (numerator / denominator).astype(bf16)

    with jax.named_scope("barsend0"):
        pl.semaphore_wait(barrier, n - 1)
        def send_row(to):
            peer = 2 * to + 1
            remote(0, att_buf.at[me], att_buf.at[me], peer, recv_sem.at[0]).start()

        outward = 1 - 2 * (pair // (pairs // 2))
        for i in range(1, pairs):
            send_row(lax.rem(pair + outward * (pairs - i) + pairs, pairs))
        pl.when(side == 0)(functools.partial(send_row, pair))
        for copy in shared_copies + gate_up_copies + [down_copy, sdown_copy]:
            copy.start()

    def lend(phase, buf, sem):
        return remote(phase, buf.at[0], buf.at[0], me + 1 - 2 * side, sem)

    lent = (lend(1, out_w, recv_sem.at[1]), lend(2, residual_ref, recv_sem.at[2]))
    with jax.named_scope("lend"):
        for copy in smalls[5:]:
            copy.wait()
        out_w_copy.wait()

        @pl.when(side == 0)
        def _():
            for copy in lent:
                copy.start()

    with jax.named_scope("prep"):
        route_scores = route_scores_ref[...]
        gate_weights = (
            route_scores / jnp.sum(route_scores, axis=0, keepdims=True) * routed_scale
        )
        expert_row = lax.broadcasted_iota(jnp.int32, (n, rows), 0)
        share = jnp.zeros((n, rows), f32)
        for k in range(routes_ref.shape[0]):
            share = share + jnp.where(
                routes_ref[k : k + 1] == expert_row, gate_weights[k : k + 1], 0.0
            )
        row_eye = lax.broadcasted_iota(jnp.int32, (rows, rows), 0) == lax.broadcasted_iota(
            jnp.int32, (rows, rows), 1
        )
        shares = [
            jnp.sum(jnp.where(row_eye, share[e : e + 1], 0.0), axis=1, keepdims=True)
            for e in range(n)
        ]

    def project():
        for copy in lent:
            copy.wait_recv()
        with jax.named_scope("arrive0"):
            arrive(0, att_buf, recv_sem.at[0], 0, n - 1)
        with jax.named_scope("oproj_send1"):
            att_wide[...] = att_buf[...].astype(f32).reshape(n * heads, head_size)
            attended = jnp.concatenate(
                [att_wide[pl.ds(h, n, stride=heads), :].astype(bf16) for h in range(heads)], axis=1
            )
            halves = []
            for k in range(2):
                mixed = jnp.dot(attended, out_w[k], preferred_element_type=f32)
                halves.append(widen((residual_ref[k].astype(f32) + mixed).astype(bf16)))
            stream_buf[pair] = widen(join_lanes(halves, width))
            block = stream_buf.at[pair]

            def send_stream(to, core):
                remote(1 + core, block, block, 2 * to + core, stream_sem.at[home]).start()

            for i in range(pairs - 1):
                last = pairs - 1 - i
                for core in range(2):
                    send_stream(last - jnp.where(last <= pair, 1, 0), core)
                if i == 0:
                    send_stream(pair, 0)

    pl.when(leads)(project)

    @pl.when(side == 0)
    def _():
        sent(0, att_buf, pairs)
        for copy in lent:
            copy.wait_send()

    def stream_sent():
        sent(0, att_buf, pairs - 1)
        sent(1, stream_buf, pairs)
        sent(2, stream_buf, pairs - 1)

    with jax.named_scope("wwait"):
        pltpu.make_async_copy(shared_w, shared_w, key_sem.at[2]).wait()
        pltpu.make_async_copy(gate_up_w, gate_up_w, key_sem.at[3]).wait()

    with jax.named_scope("gateup_send2"):
        weights = (shared_w.at[0], shared_w.at[1], gate_up_w.at[0], gate_up_w.at[1])
        sums = [jnp.zeros((rows, w.shape[0]), f32) for w in weights]
        squares = jnp.zeros((rows, 1), f32)
        firsts = (first_shared.at[0], first_shared.at[1], first_expert.at[0], first_expert.at[1])
        for i in range(turns):
            c = visit(i)
            part = pl.ds(pl.multiple_of(c * wide, wide), wide)
            with jax.named_scope("w%d" % i):
                if i == turns - 2:
                    down_copy.wait()
                    sdown_copy.wait()
                come = functools.partial(arrive, 1, stream_buf, stream_sem.at[c])
                if i:
                    come(c * pair_per, pair_per)
                else:
                    pl.when(side == 0)(functools.partial(come, 0, pair_per))
                    if pair_per > 1:
                        pl.when(leads)(functools.partial(come, 0, pair_per - 1))
            block = join_lanes(
                [stream_buf[c * pair_per + t] for t in range(pair_per)], 2 * width
            ).astype(f32)
            squares = squares + jnp.sum(block * block, axis=1, keepdims=True)
            scaled = (block * gain_ref[:, part]).astype(bf16)
            sums = [total + dot_t(scaled, w[:, part]) for total, w in zip(sums, weights)]
            if i == turns - 2:
                pl.when(leads)(stream_sent)
            if i == 0:
                for ref, total in zip(firsts, sums):
                    ref[...] = total
                sums = [jnp.zeros_like(total) for total in sums]
        sums = [ref[...] + total for ref, total in zip(firsts, sums)]
        inv_rms = lax.rsqrt(squares * (1.0 / model) + norm_eps)
        sgated, supped, gated, upped = [total * inv_rms for total in sums]

        mid_buf[me] = widen((jax.nn.silu(sgated) * supped).astype(bf16))
        for k in range(per):
            send_mid(k)
        hidden = (jax.nn.silu(gated) * upped).astype(bf16)
    with jax.named_scope("down_send3"):

        def expert_out(c):
            part = pl.ds(pl.multiple_of(c * wide, wide), wide)
            return jnp.dot(hidden, down_w[:, part], preferred_element_type=f32).astype(bf16)

        def send_block(peer):
            remote(1, eo_src.at[peer], eo_buf.at[me], peer, recv_sem.at[1]).start()

        def put(i, c, out):
            for s in range(per):
                eo_src[c * per + s] = widen(out[:, s * width : (s + 1) * width])
            if i < turns - 1:
                for s in range(per):
                    send_block(c * per + s)
            else:
                for s in range(per - 1):
                    send_block(c * per + s + jnp.where(me - c * per <= s, 1, 0))
            if i:
                for k in range(i * per, min((i + 1) * per, n - 1)):
                    send_mid(k)

        chips = [i + jnp.where(home <= i, 1, 0) for i in range(turns - 1)] + [home]
        put(0, chips[0], expert_out(chips[0]))
        out = expert_out(chips[1])
        for i in range(2, turns):
            following = expert_out(chips[i])
            put(i - 1, chips[i - 1], out)
            out = following
        put(turns - 1, home, out)
        eo_buf[me] = eo_src[me]

    with jax.named_scope("arrive2"):
        arrive(0, mid_buf, recv_sem.at[0], 0, n - 1)
    with jax.named_scope("sdown"):
        mid = jnp.concatenate([mid_buf[j] for j in range(n)], axis=1)
        shared_down = sdown_w[...].reshape(mid.shape[1], width)
        mine = stream_buf[pair].astype(f32)
        stream = jnp.where(leads, mine[:, width : 2 * width], mine[:, :width])
        total = stream + jnp.dot(mid, shared_down, preferred_element_type=f32)
    with jax.named_scope("arrive3"):
        arrive(1, eo_buf, recv_sem.at[1], 0, n - 1)
    with jax.named_scope("final"):
        for e in range(n):
            total = total + shares[e] * eo_buf[e][:, :width].astype(f32)
        out_ref[...] = total.astype(bf16)
        sent(0, mid_buf, n - 1)
        sent(1, eo_src, n - 1)


def solution(mesh):
    n = mesh.shape["ep"]

    def on_device(
        queries,
        fresh_token_key,
        value_new,
        forget_logit,
        cache_keys,
        cache_values,
        cache_cumlog,
        lengths,
        residual,
        out_weight,
        norm_gain,
        expert_gate,
        expert_up,
        expert_down,
        shared_gate,
        shared_up,
        shared_down,
        routes,
        route_scores,
    ):
        rows, width = residual.shape
        heads, head_size = queries.shape[1:]
        span = cache_keys.shape[2]
        model = norm_gain.shape[0]
        lanes = -(-width // LANES) * LANES
        mid_lanes = -(-shared_gate.shape[0] // LANES) * LANES
        pair_lanes = -(-2 * width // LANES) * LANES
        turns = model // (2 * max(width, LANES))
        chunks = 4
        hbm = pl.BlockSpec(memory_space=pltpu.HBM)

        def like(a, drop=0):
            return pltpu.VMEM(a.shape[drop:], a.dtype)

        def held(a):
            return pltpu.with_memory_space_constraint(a, pltpu.HBM)

        return pl.pallas_call(
            functools.partial(layer, n),
            out_shape=pltpu.VMEM((rows, width), bf16),
            in_specs=[pl.BlockSpec(memory_space=pl.ANY)] + [hbm] * 18,
            out_specs=pl.BlockSpec(memory_space=pltpu.VMEM),
            scratch_shapes=[
                pltpu.SMEM((1, 1), jnp.int32),
                like(queries),
                like(fresh_token_key),
                like(value_new),
                like(forget_logit),
                pltpu.VMEM((2, *residual.shape), bf16),
                pltpu.VMEM((1, model), f32),
                pltpu.VMEM(routes.shape[::-1], routes.dtype),
                pltpu.VMEM(route_scores.shape[::-1], f32),
                like(cache_keys, 1),
                like(cache_values, 1),
                like(cache_cumlog, 1),
                pltpu.VMEM((2, *out_weight.shape), bf16),
                pltpu.VMEM((2, *expert_gate.shape[1:]), bf16),
                like(expert_down, 1),
                pltpu.VMEM((2, *shared_gate.shape), bf16),
                pltpu.VMEM((n, mid_lanes, width), bf16),
                pltpu.VMEM((n, heads, head_size), bf16),
                pltpu.VMEM((n * heads, head_size), f32),
                pltpu.VMEM((n // 2, rows, pair_lanes), bf16),
                pltpu.VMEM((n, rows, mid_lanes), bf16),
                pltpu.VMEM((n, rows, lanes), bf16),
                pltpu.VMEM((n, rows, lanes), bf16),
                pltpu.VMEM((2, rows, shared_gate.shape[0]), f32),
                pltpu.VMEM((2, rows, expert_gate.shape[1]), f32),
                pltpu.SemaphoreType.DMA((5,)),
                pltpu.SemaphoreType.DMA((chunks,)),
                pltpu.SemaphoreType.DMA((2 + 1,)),
                pltpu.SemaphoreType.DMA((3,)),
                pltpu.SemaphoreType.DMA((3,)),
                pltpu.SemaphoreType.DMA((turns,)),
            ],
            compiler_params=pltpu.CompilerParams(
                collective_id=0, has_side_effects=True, vmem_limit_bytes=VMEM_LIMIT
            ),
            name="layer",
        )(
            lengths.reshape(1, 1),
            *map(
                held,
                (
                    queries,
                    fresh_token_key,
                    value_new,
                    forget_logit,
                    residual,
                    norm_gain.reshape(1, -1),
                    routes.T,
                    route_scores.T,
                    cache_keys,
                    cache_values,
                    cache_cumlog,
                    out_weight,
                    expert_gate,
                    expert_up,
                    expert_down,
                    shared_gate,
                    shared_up,
                    shared_down.reshape(n, -1, width),
                ),
            ),
        )

    placed = (
        P(("grp", "ep"), None, None),
        P(("grp", "ep"), None, None),
        P(("grp", "ep"), None, None),
        P(("grp", "ep"), None),
        P(("grp", "ep"), None, None, None),
        P(("grp", "ep"), None, None, None),
        P(("grp", "ep"), None, None),
        P(("grp", "ep")),
        P("grp", "ep"),
        P(None, "ep"),
        P(),
        P("ep", None, None),
        P("ep", None, None),
        P("ep", None, None),
        P("ep", None),
        P("ep", None),
        P(None, "ep"),
        P("grp", None),
        P("grp", None),
    )
    return jax.shard_map(
        on_device, mesh=mesh, in_specs=placed, out_specs=P("grp", "ep"), check_vma=False
    )
```
